32 devices in a mesh: ra: 4 (over z), cb: 8 (over y, x, core).
Axes of the slice: x: 2, y: 2, z: 4, core: 2. Of those that a mesh axis runs over, the one named last changes fastest.
Arguments:
- tokens: bfloat16 [2, 128, 3072], P(None, None, 'ra'), may hold values from -70 to 70
- norm_gain: float32 [2, 3072], P(None, 'ra'), may hold values from 0.1 to 1.9
- gate_weight: float32 [2, 3072, 8448], P(None, 'ra', 'cb'), may hold values from -0.109375 to 0.109375
- gate_scale: float32 [2, 8448], P(None, 'cb'), may hold values from 0.5 to 2
- up_weight: float32 [2, 3072, 8448], P(None, 'ra', 'cb'), may hold values from -0.109375 to 0.109375
- up_scale: float32 [2, 8448], P(None, 'cb'), may hold values from 0.5 to 2
- conv_weight: float32 [2, 3, 8448], P(None, None, 'cb'), may hold values from -3.5 to 3.5
- conv_bias: float32 [2, 8448], P(None, 'cb'), may hold values from -3 to 3
- down_weight: float32 [2, 8448, 3072], P(None, 'cb', 'ra'), may hold values from -0.0625 to 0.0625
- down_scale: float32 [2, 3072], P(None, 'ra'), may hold values from 0.5 to 2
Outputs:
- layer_output: bfloat16 [2, 128, 3072], P(None, None, 'ra')
The draws below stay inside these ranges and needn't reach their ends.
All inputs are finite; a program needn't handle non-finite values.
Results may differ from the reference program's by a relative error of at most 0.014.
Values may be sent and summed in bfloat16 or wider, within the bound.
A program may use at most 64 MiB of HBM per device.

```python
import math
import jax
import jax.numpy as jnp
from jax import lax

WIDTH = 3072
UNITS = 8448
KERNEL = 3
SEQUENCES = 2
LENGTH = 128


def draw_tokens(key, part):
    first, second, third = jax.random.split(key, 3)
    column_scale = jnp.exp(jnp.linspace(0.0, math.log(6.0), WIDTH)).astype(jnp.float32)
    rough = jnp.exp(jax.random.uniform(second, (WIDTH,), jnp.float32, -0.5, 0.5))
    row_scale = jnp.exp(jax.random.uniform(third, (SEQUENCES, LENGTH, 1), jnp.float32, 0.0, math.log(10.0)))
    base = jnp.clip(jax.random.normal(first, (SEQUENCES, LENGTH, WIDTH), jnp.float32), -4.0, 4.0)
    values = base * column_scale * rough * row_scale / 6.0
    return values.astype(jnp.bfloat16)


def shard_levels(key, shape, pieces, smallest, high):
    level, own = 1.0, jax.random.fold_in(key, 6)
    for position, shards_of in pieces:
        heights = jnp.exp(jax.random.uniform(jax.random.fold_in(own, position), (shards_of,), jnp.float32, smallest / len(pieces), high / len(pieces)))
        level = level * jnp.repeat(heights, shape[position] // shards_of).reshape([-1 if axis == position else 1 for axis in range(len(shape))])
    return level


def normal_values(rng, extent, deviation, most, pieces=(), held_as=jnp.bfloat16):
    gain = shard_levels(rng, extent, pieces, -0.22, 0.18) if pieces else 1.0
    drawn = jax.random.normal(rng, extent, jnp.float32) * deviation * gain
    return jnp.minimum(jnp.maximum(drawn, -most), most).astype(held_as)


def setup_inputs(seed: int = 0) -> dict:
    keys = jax.random.split(jax.random.key(seed), 11)
    tokens = draw_tokens(jax.random.fold_in(keys[10], 71), 0)
    norm_gain = jnp.clip(1.0 + 0.18 * jax.random.normal(keys[1], (2, WIDTH), jnp.float32), 0.1, 1.9)
    gate_weight = normal_values(keys[2], (2, WIDTH, UNITS), WIDTH ** -0.5, 0.109375, ((1, 4), (2, 8)), jnp.float32)
    gate_scale = jnp.clip(jnp.exp(math.log(2.0) - 1.3862944 * jax.random.uniform(keys[3], (2, UNITS), jnp.float32) ** shard_levels(keys[3], (2, UNITS), ((1, 8),), -0.2, 0.2)), 0.5, 2.0)
    up_weight = normal_values(keys[4], (2, WIDTH, UNITS), WIDTH ** -0.5, 0.109375, ((1, 4), (2, 8)), jnp.float32)
    up_scale = jnp.clip(jnp.exp(math.log(2.0) - 1.3862944 * jax.random.uniform(keys[5], (2, UNITS), jnp.float32) ** shard_levels(keys[5], (2, UNITS), ((1, 8),), -0.2, 0.2)), 0.5, 2.0)
    conv_weight = normal_values(keys[6], (2, KERNEL, UNITS), KERNEL ** -0.5, 3.5, ((2, 8),), jnp.float32)
    conv_bias = normal_values(keys[7], (2, UNITS), 0.5, 3.0, ((1, 8),), jnp.float32)
    down_weight = normal_values(keys[8], (2, UNITS, WIDTH), UNITS ** -0.5, 0.0625, ((1, 8), (2, 4)), jnp.float32)
    down_scale = jnp.clip(jnp.exp(math.log(2.0) - 1.3862944 * jax.random.uniform(keys[9], (2, WIDTH), jnp.float32) ** shard_levels(keys[9], (2, WIDTH), ((1, 4),), -0.2, 0.2)), 0.5, 2.0)
    return {"tokens": tokens, "norm_gain": norm_gain, "gate_weight": gate_weight, "gate_scale": gate_scale, "up_weight": up_weight, "up_scale": up_scale, "conv_weight": conv_weight, "conv_bias": conv_bias, "down_weight": down_weight, "down_scale": down_scale}


eps = 1e-06
residual_keep = 0.5

def causal_mix(gate_seq, conv_taps, conv_shift):
    count = conv_taps.shape[0]
    padded = jnp.pad(gate_seq, ((0, 0), (count - 1, 0), (0, 0)))
    running = jnp.zeros_like(gate_seq) + conv_shift[None, None, :]
    for offset in range(count):
        running = running + conv_taps[offset][None, None, :] * padded[:, offset:offset + LENGTH, :]
    return running

def sublayer(current, norm_g, gate_w, gate_s, up_w, up_s, conv_taps, conv_shift, down_w, down_s):
    values = current.astype(jnp.float32).reshape(SEQUENCES * LENGTH, WIDTH)
    inverse_rms = lax.rsqrt(lax.optimization_barrier(jnp.mean(values * values, axis=1, keepdims=True)) + eps)
    scaled = (values * norm_g[None, :]).astype(jnp.bfloat16)
    gate_sum = jnp.dot(scaled, gate_w.astype(jnp.bfloat16), preferred_element_type=jnp.float32)
    up_sum = jnp.dot(scaled, up_w.astype(jnp.bfloat16), preferred_element_type=jnp.float32)
    gate_sum = gate_sum * inverse_rms * gate_s[None, :]
    up_sum = up_sum * inverse_rms * up_s[None, :]
    conv_out = causal_mix(gate_sum.reshape(SEQUENCES, LENGTH, UNITS), conv_taps, conv_shift)
    hidden_act = (jax.nn.silu(conv_out) * up_sum.reshape(SEQUENCES, LENGTH, UNITS)).astype(jnp.bfloat16)
    hidden_act = hidden_act.reshape(SEQUENCES * LENGTH, UNITS)
    branch = jnp.dot(hidden_act, down_w.astype(jnp.bfloat16), preferred_element_type=jnp.float32) * down_s[None, :]
    return (residual_keep * values + branch).astype(jnp.bfloat16).reshape(SEQUENCES, LENGTH, WIDTH)

def reference(tokens, norm_gain, gate_weight, gate_scale, up_weight, up_scale, conv_weight, conv_bias, down_weight, down_scale):
    current = tokens
    for layer_index in range(2):
        current = sublayer(current, norm_gain[layer_index], gate_weight[layer_index], gate_scale[layer_index], up_weight[layer_index], up_scale[layer_index], conv_weight[layer_index], conv_bias[layer_index], down_weight[layer_index], down_scale[layer_index])
    return current
```

```python
import functools

import jax
import jax.numpy as jnp
from jax import lax
from jax.experimental import pallas as pl
from jax.experimental.pallas import tpu as pltpu
from jax.sharding import PartitionSpec as P

eps = 1e-06
residual_keep = 0.5


def causal_mix(gate_seq, conv_taps, conv_shift):
    count = conv_taps.shape[0]
    length = gate_seq.shape[1]
    padded = jnp.pad(gate_seq, ((0, 0), (count - 1, 0), (0, 0)))
    running = jnp.zeros_like(gate_seq) + conv_shift[None, None, :]
    for offset in range(count):
        running = (
            running + conv_taps[offset][None, None, :] * padded[:, offset : offset + length, :]
        )
    return running


def sublayer(current, norm_g, gate_w, gate_s, up_w, up_s, conv_taps, conv_shift, down_w, down_s):
    sequences, length, local_width = current.shape
    row_count = sequences * length
    values = current.astype(jnp.float32).reshape(row_count, local_width)
    squares = jnp.sum(values * values, axis=1)
    scaled = (values * norm_g[None, :]).astype(jnp.bfloat16)
    gate_part = jnp.dot(scaled, gate_w.astype(jnp.bfloat16), preferred_element_type=jnp.float32)
    up_part = jnp.dot(scaled, up_w.astype(jnp.bfloat16), preferred_element_type=jnp.float32)
    gate_sum, up_sum = (
        lax.psum_scatter(gate_part, "ra", scatter_dimension=1, tiled=True),
        lax.psum_scatter(up_part, "ra", scatter_dimension=1, tiled=True),
    )
    square_sum = lax.psum(squares, "ra")
    share_cols = gate_sum.shape[1]
    col_start = lax.axis_index("ra") * share_cols
    col_gate = lax.dynamic_slice_in_dim(gate_s, col_start, share_cols, 0)
    col_up = lax.dynamic_slice_in_dim(up_s, col_start, share_cols, 0)
    used_taps = lax.dynamic_slice_in_dim(conv_taps, col_start, share_cols, 1)
    used_shift = lax.dynamic_slice_in_dim(conv_shift, col_start, share_cols, 0)
    inverse_rms = lax.rsqrt(square_sum / (local_width * lax.axis_size("ra")) + eps)[:, None]
    gate_sum = gate_sum * inverse_rms * col_gate[None, :]
    up_sum = up_sum * inverse_rms * col_up[None, :]
    units = gate_sum.shape[1]
    conv_out = causal_mix(gate_sum.reshape(sequences, length, units), used_taps, used_shift)
    hidden_act = (jax.nn.silu(conv_out) * up_sum.reshape(sequences, length, units)).astype(
        jnp.bfloat16
    )
    hidden_act = hidden_act.reshape(row_count, units)
    hidden_act = lax.all_gather(hidden_act, "ra", axis=1, tiled=True)
    down_part = jnp.dot(hidden_act, down_w.astype(jnp.bfloat16), preferred_element_type=jnp.float32)
    down_sum = lax.psum(down_part, "cb")
    branch = down_sum * down_s[None, :]
    return (
        (residual_keep * values + branch)
        .astype(jnp.bfloat16)
        .reshape(sequences, length, local_width)
    )


def shards(
    tokens,
    norm_gain,
    gate_weight,
    gate_scale,
    up_weight,
    up_scale,
    conv_weight,
    conv_bias,
    down_weight,
    down_scale,
):
    current = tokens
    for layer_index in range(2):
        current = sublayer(
            current,
            norm_gain[layer_index],
            gate_weight[layer_index],
            gate_scale[layer_index],
            up_weight[layer_index],
            up_scale[layer_index],
            conv_weight[layer_index],
            conv_bias[layer_index],
            down_weight[layer_index],
            down_scale[layer_index],
        )
    return current


MESH = pl.DeviceIdType.MESH
LANES = 128
CHUNKS = 8
PLAN = (
    ("enter", 0),
    ("act", 3),
    ("pair", 5),
    ("fold", 6),
    ("mix", 1),
    ("down", 4),
    ("done", 6),
)
CONVERT = {1: ("out", 0), 3: ("in", 1), 5: ("out", 1)}


def fused(
    chunks,
    ra,
    cb,
    tokens_hbm,
    norm_gain_hbm,
    gate_weight,
    gate_scale_hbm,
    up_weight,
    up_scale_hbm,
    conv_weight_hbm,
    conv_bias_hbm,
    down_weight,
    down_scale_hbm,
    out,
    stage_gate,
    stage_up,
    stage_down,
    norm_gain,
    gate_scale,
    up_scale,
    conv_weight,
    conv_bias,
    down_scale,
    in_w,
    out_w,
    state,
    own_part,
    near_part,
    far_send,
    far_part,
    hidden,
    down_keep,
    pair_send,
    pair_recv,
    chip_part,
    conv_pad,
    params,
    load_sem,
    small_sem,
    token_sem,
    near_s,
    near_r,
    far_s,
    far_r,
    hid_s,
    hid_r,
    pair_s,
    pair_r,
    chip_s,
    chip_r,
    out_s,
    out_r,
):
    layers = 2
    sequences, length, width = tokens_hbm.shape
    units = gate_weight.shape[1]
    main = units // LANES * LANES
    rem = units - main
    total_cols = 2 * main + LANES
    step = length // chunks
    rows = sequences * step
    items = layers * chunks
    half = width // 2
    chips = cb // 2
    split = main // 2
    me = lax.axis_index("ra")
    mine = lax.axis_index("cb")
    core = lax.rem(mine, 2)
    chip = mine // 2
    inner = jnp.logical_and(me >= 1, me <= 2)
    outer = jnp.logical_not(inner)
    own_seq = me - 1
    my_cols = pl.ds(pl.multiple_of(core * half, LANES), half)
    other_cols = pl.ds(pl.multiple_of((1 - core) * half, LANES), half)

    barrier = pltpu.get_barrier_semaphore()
    for d in range(1, ra):
        to = lax.rem(me + d, ra)

        @pl.when(jnp.logical_or(inner, jnp.logical_and(to >= 1, to <= 2)))
        def _():
            pl.semaphore_signal(barrier, inc=1, device_id={"ra": to}, device_id_type=MESH)

    pl.semaphore_signal(
        barrier, inc=1, device_id={"cb": 2 * chip + 1 - core}, device_id_type=MESH
    )
    for d in range(1, chips):
        pl.semaphore_signal(
            barrier,
            inc=1,
            device_id={"cb": 2 * lax.rem(chip + d, chips) + core},
            device_id_type=MESH,
        )

    def token_copy(c, s):
        return pltpu.make_async_copy(
            tokens_hbm.at[s, pl.ds(pl.multiple_of(c * step, step), step)],
            state.at[c, pl.ds(s * step, step)],
            token_sem.at[c, s],
        )

    smalls = [
        pltpu.make_async_copy(src, dst, small_sem.at[i])
        for i, (src, dst) in enumerate(
            (
                (norm_gain_hbm, norm_gain),
                (gate_scale_hbm, gate_scale),
                (up_scale_hbm, up_scale),
                (conv_weight_hbm, conv_weight),
                (conv_bias_hbm, conv_bias),
                (down_scale_hbm, down_scale),
            )
        )
    ]
    pieces = ((0, split), (split, units - split))

    def load(layer, kind, part):
        src, dst = (
            (gate_weight, stage_gate),
            (up_weight, stage_up),
            (down_weight, stage_down),
        )[kind]
        r = pl.ds(*pieces[part])
        return pltpu.make_async_copy(
            src.at[layer, r], dst.at[layer, r], load_sem.at[layer * 6 + kind * 2 + part]
        )

    for s in range(sequences):
        token_copy(0, s).start()
    smalls[0].start()
    for part in range(2):
        for kind in range(2):
            load(0, kind, part).start()
    for copy in smalls[1:]:
        copy.start()
    for c in range(1, chunks):
        for s in range(sequences):
            token_copy(c, s).start()
    for part in range(2):
        load(0, 2, part).start()
    for kind in range(3):
        for part in range(2):
            load(1, kind, part).start()

    block = 32

    def convert_piece(layer, kind, part):
        load(layer, kind, part).wait()
        src = (stage_gate, stage_up)[kind]
        first, stop = part * split, (part + 1) * split

        @pl.loop(first // block, stop // block)
        def _(i):
            r = pl.ds(pl.multiple_of(i * block, block), block)
            r2 = pl.ds(pl.multiple_of(kind * main + i * block, block), block)
            in_w[layer, r2, :] = src[layer, r, :].astype(jnp.bfloat16)

        if rem and part:
            first = 2 * main + kind * rem
            in_w[layer, first : first + rem, :] = src[layer, main:, :].astype(jnp.bfloat16)

    def convert_in(layer):
        for part in range(2):
            for kind in range(2):
                convert_piece(layer, kind, part)
        first = 2 * main + 2 * rem
        in_w[layer, first:, :] = jnp.zeros((LANES - 2 * rem, width), jnp.bfloat16)

    def convert_out(layer):
        for part in range(2):
            load(layer, 2, part).wait()

        @pl.loop(0, units // block)
        def _(i):
            r = pl.ds(pl.multiple_of(i * block, block), block)
            out_w[layer, r, :half] = stage_down[layer, r, other_cols].astype(jnp.bfloat16)
            out_w[layer, r, half:] = stage_down[layer, r, my_cols].astype(jnp.bfloat16)

        pad = out_w.shape[1] - units
        if pad:
            out_w[layer, units:, :] = jnp.zeros((pad, width), jnp.bfloat16)

    lane = lax.broadcasted_iota(jnp.int32, (1, LANES), 1)

    def put_squares(tile, squares):
        high = squares.astype(jnp.bfloat16).astype(jnp.float32)
        low = squares - high
        return jnp.where(lane == 2 * rem, high, jnp.where(lane == 2 * rem + 1, low, tile))

    def get_squares(tile):
        keep = jnp.logical_and(lane >= 2 * rem, lane < 2 * rem + 2)
        return jnp.sum(jnp.where(keep, tile, 0.0), axis=1, keepdims=True)

    def near_copy(k, first):
        to = jnp.where(me == 0, 1, 2)
        passed = jnp.where(me < 2, 1, 0)
        r = hid_rows(passed if first else 1 - passed)
        return pltpu.make_async_remote_copy(
            src_ref=own_part.at[k, r],
            dst_ref=near_part.at[k, r],
            send_sem=near_s.at[k, int(first)],
            recv_sem=near_r.at[k, int(first)],
            device_id={"ra": to},
            device_id_type=MESH,
        )

    def far_copy(k):
        return pltpu.make_async_remote_copy(
            src_ref=far_send.at[k],
            dst_ref=far_part.at[k],
            send_sem=far_s.at[k],
            recv_sem=far_r.at[k],
            device_id={"ra": 3 - me},
            device_id_type=MESH,
        )

    def hid_rows(seq):
        return pl.ds(pl.multiple_of(seq * step, step), step)

    def hid_copy(k, d, seq):
        return pltpu.make_async_remote_copy(
            src_ref=hidden.at[k, hid_rows(seq)],
            dst_ref=hidden.at[k, hid_rows(seq)],
            send_sem=hid_s.at[k, d - 1],
            recv_sem=hid_r.at[k, seq],
            device_id={"ra": lax.rem(me + d, ra)},
            device_id_type=MESH,
        )

    def pair_copy(k):
        return pltpu.make_async_remote_copy(
            src_ref=pair_send.at[k],
            dst_ref=pair_recv.at[k],
            send_sem=pair_s.at[k],
            recv_sem=pair_r.at[k],
            device_id={"cb": 2 * chip + 1 - core},
            device_id_type=MESH,
        )

    def chip_copy(k, d):
        return pltpu.make_async_remote_copy(
            src_ref=chip_part.at[k, chip],
            dst_ref=chip_part.at[k, chip],
            send_sem=chip_s.at[k, d - 1],
            recv_sem=chip_r.at[k, d - 1],
            device_id={"cb": 2 * lax.rem(chip + d, chips) + core},
            device_id_type=MESH,
        )

    def chip_wait(k, d):
        return pltpu.make_async_remote_copy(
            src_ref=chip_part.at[k, chip],
            dst_ref=chip_part.at[k, lax.rem(chip - d + chips, chips)],
            send_sem=chip_s.at[k, d - 1],
            recv_sem=chip_r.at[k, d - 1],
            device_id={"cb": 2 * lax.rem(chip + d, chips) + core},
            device_id_type=MESH,
        )

    def out_copy(k, cols):
        return pltpu.make_async_remote_copy(
            src_ref=state.at[k + chunks, :, cols],
            dst_ref=state.at[k + chunks, :, cols],
            send_sem=out_s.at[k],
            recv_sem=out_r.at[k],
            device_id={"cb": 2 * chip + 1 - core},
            device_id_type=MESH,
        )

    def project(k):
        layer = k // chunks

        @pl.when(k < chunks)
        def _():
            for s in range(sequences):
                token_copy(k, s).wait()

        values = state[k].astype(jnp.float32)
        squares = jnp.sum(values * values, axis=1, keepdims=True)
        gain = norm_gain[pl.ds(layer, 1), :]
        scaled = (values * gain).astype(jnp.bfloat16)
        cols = 512
        for start in range(0, 2 * main, cols):
            stop = min(start + cols, 2 * main)
            own_part[k, :, start:stop] = lax.dot_general(
                scaled,
                in_w[layer, start:stop, :],
                (((1,), (1,)), ((), ())),
                preferred_element_type=jnp.float32,
            ).astype(jnp.bfloat16)
        tile = lax.dot_general(
            scaled,
            in_w[layer, 2 * main :, :],
            (((1,), (1,)), ((), ())),
            preferred_element_type=jnp.float32,
        )
        own_part[k, :, 2 * main :] = put_squares(tile, squares).astype(jnp.bfloat16)

    def enter(k):
        @pl.when(k > 0)
        def _():
            project(k)

        @pl.when(outer)
        def _():
            near_copy(k, True).start()
            near_copy(k, False).start()

    def mix(k):
        near_copy(k, True).wait_recv()
        r = hid_rows(1 - own_seq)
        both = own_part[k, r, : 2 * main].astype(jnp.float32) + near_part[
            k, r, : 2 * main
        ].astype(jnp.float32)
        far_send[k, :, : 2 * main] = both.astype(jnp.bfloat16)
        tile = own_part[k, r, 2 * main :].astype(jnp.float32) + near_part[k, r, 2 * main :].astype(
            jnp.float32
        )
        far_send[k, :, 2 * main :] = put_squares(tile, get_squares(tile)).astype(jnp.bfloat16)
        far_copy(k).start()

    def act(k):
        layer = k // chunks
        near_copy(k, False).wait_recv()
        far_copy(k).wait_recv()
        r = hid_rows(own_seq)

        def total(start, stop):
            return (
                own_part[k, r, start:stop].astype(jnp.float32)
                + near_part[k, r, start:stop].astype(jnp.float32)
                + far_part[k, :, start:stop].astype(jnp.float32)
            )

        tile = total(2 * main, total_cols)
        inverse_rms = lax.rsqrt(get_squares(tile) / (width * ra) + eps)

        @pl.when(k % chunks == 0)
        def _():
            conv_pad[0:8, :] = jnp.zeros((8, conv_pad.shape[1]), jnp.float32)

        def piece(gate, up, start, stop):
            def param(row):
                return params[layer, row : row + 1, start:stop]

            conv_pad[8 : 8 + step, start:stop] = gate * inverse_rms * param(0)
            conv = param(2)
            taps = conv_weight.shape[0]
            for j in range(taps):
                first = 8 - (taps - 1) + j
                conv = conv + param(3 + j) * conv_pad[first : first + step, start:stop]
            conv_pad[0:8, start:stop] = conv_pad[step : step + 8, start:stop]
            value = conv / (1.0 + jnp.exp(-conv)) * (up * inverse_rms * param(1))
            hidden[k, r, start:stop] = value.astype(jnp.bfloat16)

        cols = 256
        for start in range(0, main, cols):
            stop = min(start + cols, main)
            piece(total(start, stop), total(main + start, main + stop), start, stop)
        if rem:
            piece(tile, pltpu.roll(tile, LANES - rem, axis=1), main, main + LANES)
        for d in (2, 1, 3):
            hid_copy(k, d, own_seq).start()

    def down(k):
        layer = k // chunks
        for seq in range(sequences):

            @pl.when(jnp.logical_not(jnp.logical_and(inner, own_seq == seq)))
            def _():
                hid_copy(k, 1, seq).wait_recv()

        value = jnp.dot(hidden[k], out_w[layer], preferred_element_type=jnp.float32)
        pair_send[k] = value[:, :half].astype(jnp.bfloat16)
        down_keep[k] = value[:, half:]
        pair_copy(k).start()

    def pair(k):
        pair_copy(k).wait_recv()
        chip_part[k, chip] = (down_keep[k] + pair_recv[k].astype(jnp.float32)).astype(jnp.bfloat16)
        for d in range(1, chips):
            chip_copy(k, d).start()

    def fold(k):
        layer = k // chunks
        for d in range(1, chips):
            chip_wait(k, d).wait_recv()
        total = chip_part[k, 0].astype(jnp.float32)
        for g in range(1, chips):
            total = total + chip_part[k, g].astype(jnp.float32)
        kept = residual_keep * state[k, :, my_cols].astype(jnp.float32)
        scale = down_scale[pl.ds(layer, 1), my_cols]
        state[k + chunks, :, my_cols] = (kept + total * scale).astype(jnp.bfloat16)
        out_copy(k, my_cols).start()

    def done(k):
        out_copy(k, other_cols).wait_recv()

        @pl.when(k >= chunks)
        def _():
            for s in range(sequences):
                c = pl.ds(pl.multiple_of((k - chunks) * step, step), step)
                out[s, c, :] = state[k + chunks, s * step : (s + 1) * step, :]

    smalls[0].wait()
    convert_in(0)
    project(0)
    pl.semaphore_wait(barrier, jnp.where(inner, ra - 1, ra - 2) + chips)

    works = dict(
        enter=enter, mix=mix, act=act, down=down, pair=pair, fold=fold, done=done
    )

    def prepare():
        for copy in smalls[1:]:
            copy.wait()
        for layer in range(layers):
            lines = [gate_scale[layer : layer + 1, :], up_scale[layer : layer + 1, :]]
            lines.append(conv_bias[layer : layer + 1, :])
            lines += [conv_weight[j, layer : layer + 1, :] for j in range(conv_weight.shape[0])]
            for row, line in enumerate(lines):
                if rem:
                    zeros = jnp.zeros((1, LANES - rem), jnp.float32)
                    params[layer, row : row + 1, main:] = jnp.concatenate(
                        [line[:, main:], zeros], axis=1
                    )
                params[layer, row : row + 1, :main] = line[:, :main]

    @pl.loop(0, items + max(lag for _, lag in PLAN))
    def _(slot):
        for name, lag in PLAN:
            item = slot - lag
            good = jnp.logical_and(item >= 0, item < items)
            if name in ("mix", "act"):
                good = jnp.logical_and(good, inner)

            @pl.when(good)
            def _():
                works[name](item)

            if name == "enter":

                @pl.when(slot == 0)
                def _():
                    prepare()

                for at, (kind, layer) in CONVERT.items():

                    @pl.when(slot == at)
                    def _():
                        (convert_in if kind == "in" else convert_out)(layer)

    @pl.loop(0, items)
    def _(k):
        @pl.when(outer)
        def _():
            near_copy(k, True).wait_send()
            near_copy(k, False).wait_send()

        @pl.when(inner)
        def _():
            far_copy(k).wait_send()
            for d in range(1, ra):
                hid_copy(k, d, own_seq).wait_send()

        pair_copy(k).wait_send()
        for d in range(1, chips):
            chip_copy(k, d).wait_send()
        out_copy(k, my_cols).wait_send()


def fused_shards(ra, cb, chunks, *operands):
    tokens, gate_weight = operands[0], operands[2]
    layers = 2
    sequences, length, width = tokens.shape
    units = gate_weight.shape[2]
    main = units // LANES * LANES
    total_cols = 2 * main + LANES
    padded = main + (LANES if units > main else 0)
    step = length // chunks
    rows = sequences * step
    items = layers * chunks
    half = width // 2
    chips = cb // 2
    taps = operands[6].shape[1]
    hbm = pl.BlockSpec(memory_space=pl.ANY)
    dma = pltpu.SemaphoreType.DMA
    bf16, f32 = jnp.bfloat16, jnp.float32
    return pl.pallas_call(
        functools.partial(fused, chunks, ra, cb),
        out_shape=pltpu.VMEM(tokens.shape, tokens.dtype),
        in_specs=[hbm] * 10,
        out_specs=pl.BlockSpec(memory_space=pltpu.VMEM),
        scratch_shapes=[
            pltpu.VMEM((layers, units, width), f32),
            pltpu.VMEM((layers, units, width), f32),
            pltpu.VMEM((layers, units, width), f32),
            pltpu.VMEM((layers, width), f32),
            pltpu.VMEM((layers, units), f32),
            pltpu.VMEM((layers, units), f32),
            pltpu.VMEM((taps, layers, units), f32),
            pltpu.VMEM((layers, units), f32),
            pltpu.VMEM((layers, width), f32),
            pltpu.VMEM((layers, total_cols, width), bf16),
            pltpu.VMEM((layers, padded, width), bf16),
            pltpu.VMEM((items + chunks, rows, width), bf16),
            pltpu.VMEM((items, rows, total_cols), bf16),
            pltpu.VMEM((items, rows, total_cols), bf16),
            pltpu.VMEM((items, step, total_cols), bf16),
            pltpu.VMEM((items, step, total_cols), bf16),
            pltpu.VMEM((items, rows, padded), bf16),
            pltpu.VMEM((items, rows, half), f32),
            pltpu.VMEM((items, rows, half), bf16),
            pltpu.VMEM((items, rows, half), bf16),
            pltpu.VMEM((items, chips, rows, half), bf16),
            pltpu.VMEM((8 + step, padded), f32),
            pltpu.VMEM((layers, 3 + taps, padded), f32),
            dma((layers * 6,)),
            dma((6,)),
            dma((chunks, sequences)),
            dma((items, sequences)),
            dma((items, sequences)),
            dma((items,)),
            dma((items,)),
            dma((items, ra - 1)),
            dma((items, sequences)),
            dma((items,)),
            dma((items,)),
            dma((items, chips - 1)),
            dma((items, chips - 1)),
            dma((items,)),
            dma((items,)),
        ],
        compiler_params=pltpu.CompilerParams(
            collective_id=0, has_side_effects=True, vmem_limit_bytes=60 * 1024 * 1024
        ),
    )(
        *operands[:2],
        jnp.swapaxes(gate_weight, 1, 2),
        operands[3],
        jnp.swapaxes(operands[4], 1, 2),
        operands[5],
        jnp.swapaxes(operands[6], 0, 1),
        *operands[7:],
    )


def fits(ra, cb, chunks, shape, local_width, local_units):
    rem = local_units % LANES
    return (
        ra == 4
        and cb % 2 == 0
        and cb >= 4
        and shape[0] == 2
        and shape[1] % (chunks * 16) == 0
        and local_width % (2 * LANES) == 0
        and local_units % 32 == 0
        and 2 * rem + 2 <= LANES
        and local_units >= 2 * LANES
    )


def either(ra, cb, *operands):
    tokens, gate_weight = operands[0], operands[2]
    if fits(ra, cb, CHUNKS, tokens.shape, tokens.shape[2], gate_weight.shape[2]):
        return fused_shards(ra, cb, CHUNKS, *operands)
    return shards(*operands)


def solution(mesh):
    in_specs = (
        P(None, None, "ra"),
        P(None, "ra"),
        P(None, "ra", "cb"),
        P(None, "cb"),
        P(None, "ra", "cb"),
        P(None, "cb"),
        P(None, None, "cb"),
        P(None, "cb"),
        P(None, "cb", "ra"),
        P(None, "ra"),
    )
    out_specs = P(None, None, "ra")
    return jax.shard_map(
        functools.partial(either, mesh.shape["ra"], mesh.shape["cb"]),
        mesh=mesh,
        in_specs=in_specs,
        out_specs=out_specs,
        check_vma=False,
    )
```

```python
import functools

import jax
import jax.numpy as jnp
from jax import lax
from jax.experimental import pallas as pl
from jax.experimental.pallas import tpu as pltpu
from jax.sharding import PartitionSpec as P

eps = 1e-06
residual_keep = 0.5


def causal_mix(gate_seq, conv_taps, conv_shift):
    count = conv_taps.shape[0]
    length = gate_seq.shape[1]
    padded = jnp.pad(gate_seq, ((0, 0), (count - 1, 0), (0, 0)))
    running = jnp.zeros_like(gate_seq) + conv_shift[None, None, :]
    for offset in range(count):
        running = (
            running + conv_taps[offset][None, None, :] * padded[:, offset : offset + length, :]
        )
    return running


def sublayer(current, norm_g, gate_w, gate_s, up_w, up_s, conv_taps, conv_shift, down_w, down_s):
    sequences, length, local_width = current.shape
    row_count = sequences * length
    values = current.astype(jnp.float32).reshape(row_count, local_width)
    squares = jnp.sum(values * values, axis=1)
    scaled = (values * norm_g[None, :]).astype(jnp.bfloat16)
    gate_part = jnp.dot(scaled, gate_w.astype(jnp.bfloat16), preferred_element_type=jnp.float32)
    up_part = jnp.dot(scaled, up_w.astype(jnp.bfloat16), preferred_element_type=jnp.float32)
    gate_sum, up_sum = (
        lax.psum_scatter(gate_part, "ra", scatter_dimension=1, tiled=True),
        lax.psum_scatter(up_part, "ra", scatter_dimension=1, tiled=True),
    )
    square_sum = lax.psum(squares, "ra")
    share_cols = gate_sum.shape[1]
    col_start = lax.axis_index("ra") * share_cols
    col_gate = lax.dynamic_slice_in_dim(gate_s, col_start, share_cols, 0)
    col_up = lax.dynamic_slice_in_dim(up_s, col_start, share_cols, 0)
    used_taps = lax.dynamic_slice_in_dim(conv_taps, col_start, share_cols, 1)
    used_shift = lax.dynamic_slice_in_dim(conv_shift, col_start, share_cols, 0)
    inverse_rms = lax.rsqrt(square_sum / (local_width * lax.axis_size("ra")) + eps)[:, None]
    gate_sum = gate_sum * inverse_rms * col_gate[None, :]
    up_sum = up_sum * inverse_rms * col_up[None, :]
    units = gate_sum.shape[1]
    conv_out = causal_mix(gate_sum.reshape(sequences, length, units), used_taps, used_shift)
    hidden_act = (jax.nn.silu(conv_out) * up_sum.reshape(sequences, length, units)).astype(
        jnp.bfloat16
    )
    hidden_act = hidden_act.reshape(row_count, units)
    hidden_act = lax.all_gather(hidden_act, "ra", axis=1, tiled=True)
    down_part = jnp.dot(hidden_act, down_w.astype(jnp.bfloat16), preferred_element_type=jnp.float32)
    down_sum = lax.psum(down_part, "cb")
    branch = down_sum * down_s[None, :]
    return (
        (residual_keep * values + branch)
        .astype(jnp.bfloat16)
        .reshape(sequences, length, local_width)
    )


def shards(
    tokens,
    norm_gain,
    gate_weight,
    gate_scale,
    up_weight,
    up_scale,
    conv_weight,
    conv_bias,
    down_weight,
    down_scale,
):
    current = tokens
    for layer_index in range(2):
        current = sublayer(
            current,
            norm_gain[layer_index],
            gate_weight[layer_index],
            gate_scale[layer_index],
            up_weight[layer_index],
            up_scale[layer_index],
            conv_weight[layer_index],
            conv_bias[layer_index],
            down_weight[layer_index],
            down_scale[layer_index],
        )
    return current


MESH = pl.DeviceIdType.MESH
LANES = 128
CHUNKS = 8
PLAN = (('done', 8), ('act', 3), ('enter', 0), ('pair', 5), ('fold', 7), ('mix', 1), ('down', 4))
CONVERT = {1: ("out", 0), 3: ("in", 1), 5: ("out", 1)}


def fused(
    chunks,
    ra,
    cb,
    tokens_hbm,
    norm_gain_hbm,
    gate_weight,
    gate_scale_hbm,
    up_weight,
    up_scale_hbm,
    conv_weight_hbm,
    conv_bias_hbm,
    down_weight,
    down_scale_hbm,
    out,
    stage_gate,
    stage_up,
    stage_down,
    norm_gain,
    gate_scale,
    up_scale,
    conv_weight,
    conv_bias,
    down_scale,
    in_w,
    out_w,
    state,
    own_part,
    near_part,
    far_send,
    far_part,
    hidden,
    down_keep,
    pair_send,
    pair_recv,
    chip_part,
    conv_pad,
    params,
    load_sem,
    small_sem,
    token_sem,
    near_s,
    near_r,
    far_s,
    far_r,
    hid_s,
    hid_r,
    pair_s,
    pair_r,
    chip_s,
    chip_r,
    out_s,
    out_r,
):
    layers = 2
    sequences, length, width = tokens_hbm.shape
    units = gate_weight.shape[1]
    main = units // LANES * LANES
    rem = units - main
    total_cols = 2 * main + LANES
    step = length // chunks
    rows = sequences * step
    items = layers * chunks
    half = width // 2
    chips = cb // 2
    split = main // 2
    me = lax.axis_index("ra")
    mine = lax.axis_index("cb")
    core = lax.rem(mine, 2)
    chip = mine // 2
    inner = jnp.logical_and(me >= 1, me <= 2)
    outer = jnp.logical_not(inner)
    own_seq = me - 1
    my_cols = pl.ds(pl.multiple_of(core * half, LANES), half)
    other_cols = pl.ds(pl.multiple_of((1 - core) * half, LANES), half)

    barrier = pltpu.get_barrier_semaphore()
    for d in range(1, ra):
        to = lax.rem(me + d, ra)

        @pl.when(jnp.logical_or(inner, jnp.logical_and(to >= 1, to <= 2)))
        def _():
            pl.semaphore_signal(barrier, inc=1, device_id={"ra": to}, device_id_type=MESH)

    pl.semaphore_signal(
        barrier, inc=1, device_id={"cb": 2 * chip + 1 - core}, device_id_type=MESH
    )
    for d in range(1, chips):
        pl.semaphore_signal(
            barrier,
            inc=1,
            device_id={"cb": 2 * lax.rem(chip + d, chips) + core},
            device_id_type=MESH,
        )

    def token_copy(c, s):
        return pltpu.make_async_copy(
            tokens_hbm.at[s, pl.ds(pl.multiple_of(c * step, step), step)],
            state.at[c, pl.ds(s * step, step)],
            token_sem.at[c, s],
        )

    smalls = [
        pltpu.make_async_copy(src, dst, small_sem.at[i])
        for i, (src, dst) in enumerate(
            (
                (norm_gain_hbm, norm_gain),
                (gate_scale_hbm, gate_scale),
                (up_scale_hbm, up_scale),
                (conv_weight_hbm, conv_weight),
                (conv_bias_hbm, conv_bias),
                (down_scale_hbm, down_scale),
            )
        )
    ]
    pieces = ((0, split), (split, units - split))

    def load(layer, kind, part):
        src, dst = (
            (gate_weight, stage_gate),
            (up_weight, stage_up),
            (down_weight, stage_down),
        )[kind]
        r = pl.ds(*pieces[part])
        return pltpu.make_async_copy(
            src.at[layer, r], dst.at[layer, r], load_sem.at[layer * 6 + kind * 2 + part]
        )

    for s in range(sequences):
        token_copy(0, s).start()
    smalls[0].start()
    for part in range(2):
        for kind in range(2):
            load(0, kind, part).start()
    for copy in smalls[1:]:
        copy.start()
    for c in range(1, chunks):
        for s in range(sequences):
            token_copy(c, s).start()

    block = 32

    def convert_piece(layer, kind, part):
        load(layer, kind, part).wait()
        src = (stage_gate, stage_up)[kind]
        first, stop = part * split, (part + 1) * split

        @pl.loop(first // block, stop // block)
        def _(i):
            r = pl.ds(pl.multiple_of(i * block, block), block)
            r2 = pl.ds(pl.multiple_of(kind * main + i * block, block), block)
            in_w[layer, r2, :] = src[layer, r, :].astype(jnp.bfloat16)

        if rem and part:
            first = 2 * main + kind * rem
            in_w[layer, first : first + rem, :] = src[layer, main:, :].astype(jnp.bfloat16)

    def convert_in(layer):
        for part in range(2):
            for kind in range(2):
                convert_piece(layer, kind, part)
        first = 2 * main + 2 * rem
        in_w[layer, first:, :] = jnp.zeros((LANES - 2 * rem, width), jnp.bfloat16)

    def convert_out(layer):
        for part in range(2):
            load(layer, 2, part).wait()

        @pl.loop(0, units // block)
        def _(i):
            r = pl.ds(pl.multiple_of(i * block, block), block)
            out_w[layer, r, :half] = stage_down[layer, r, other_cols].astype(jnp.bfloat16)
            out_w[layer, r, half:] = stage_down[layer, r, my_cols].astype(jnp.bfloat16)

        pad = out_w.shape[1] - units
        if pad:
            out_w[layer, units:, :] = jnp.zeros((pad, width), jnp.bfloat16)

    lane = lax.broadcasted_iota(jnp.int32, (1, LANES), 1)

    def put_squares(tile, squares):
        high = squares.astype(jnp.bfloat16).astype(jnp.float32)
        low = squares - high
        return jnp.where(lane == 2 * rem, high, jnp.where(lane == 2 * rem + 1, low, tile))

    def get_squares(tile):
        keep = jnp.logical_and(lane >= 2 * rem, lane < 2 * rem + 2)
        return jnp.sum(jnp.where(keep, tile, 0.0), axis=1, keepdims=True)

    def near_copy(k, first):
        to = jnp.where(me == 0, 1, 2)
        passed = jnp.where(me < 2, 1, 0)
        r = hid_rows(passed if first else 1 - passed)
        return pltpu.make_async_remote_copy(
            src_ref=own_part.at[k, r],
            dst_ref=near_part.at[k, r],
            send_sem=near_s.at[k, int(first)],
            recv_sem=near_r.at[k, int(first)],
            device_id={"ra": to},
            device_id_type=MESH,
        )

    def far_copy(k):
        return pltpu.make_async_remote_copy(
            src_ref=far_send.at[k],
            dst_ref=far_part.at[k],
            send_sem=far_s.at[k],
            recv_sem=far_r.at[k],
            device_id={"ra": 3 - me},
            device_id_type=MESH,
        )

    def hid_rows(seq):
        return pl.ds(pl.multiple_of(seq * step, step), step)

    def hid_copy(k, d, seq):
        return pltpu.make_async_remote_copy(
            src_ref=hidden.at[k, hid_rows(seq)],
            dst_ref=hidden.at[k, hid_rows(seq)],
            send_sem=hid_s.at[k, d - 1],
            recv_sem=hid_r.at[k, seq],
            device_id={"ra": lax.rem(me + d, ra)},
            device_id_type=MESH,
        )

    def pair_copy(k):
        return pltpu.make_async_remote_copy(
            src_ref=pair_send.at[k],
            dst_ref=pair_recv.at[k],
            send_sem=pair_s.at[k],
            recv_sem=pair_r.at[k],
            device_id={"cb": 2 * chip + 1 - core},
            device_id_type=MESH,
        )

    def chip_copy(k, d):
        return pltpu.make_async_remote_copy(
            src_ref=chip_part.at[k, chip],
            dst_ref=chip_part.at[k, chip],
            send_sem=chip_s.at[k, d - 1],
            recv_sem=chip_r.at[k, d - 1],
            device_id={"cb": 2 * lax.rem(chip + d, chips) + core},
            device_id_type=MESH,
        )

    def chip_wait(k, d):
        return pltpu.make_async_remote_copy(
            src_ref=chip_part.at[k, chip],
            dst_ref=chip_part.at[k, lax.rem(chip - d + chips, chips)],
            send_sem=chip_s.at[k, d - 1],
            recv_sem=chip_r.at[k, d - 1],
            device_id={"cb": 2 * lax.rem(chip + d, chips) + core},
            device_id_type=MESH,
        )

    def out_copy(k, cols):
        return pltpu.make_async_remote_copy(
            src_ref=state.at[k + chunks, :, cols],
            dst_ref=state.at[k + chunks, :, cols],
            send_sem=out_s.at[k],
            recv_sem=out_r.at[k],
            device_id={"cb": 2 * chip + 1 - core},
            device_id_type=MESH,
        )

    def project(k):
        layer = k // chunks

        @pl.when(k < chunks)
        def _():
            for s in range(sequences):
                token_copy(k, s).wait()

        values = state[k].astype(jnp.float32)
        squares = jnp.sum(values * values, axis=1, keepdims=True)
        gain = norm_gain[pl.ds(layer, 1), :]
        scaled = (values * gain).astype(jnp.bfloat16)
        cols = 512
        for start in range(0, 2 * main, cols):
            stop = min(start + cols, 2 * main)
            own_part[k, :, start:stop] = lax.dot_general(
                scaled,
                in_w[layer, start:stop, :],
                (((1,), (1,)), ((), ())),
                preferred_element_type=jnp.float32,
            ).astype(jnp.bfloat16)
        tile = lax.dot_general(
            scaled,
            in_w[layer, 2 * main :, :],
            (((1,), (1,)), ((), ())),
            preferred_element_type=jnp.float32,
        )
        own_part[k, :, 2 * main :] = put_squares(tile, squares).astype(jnp.bfloat16)

    def enter(k):
        @pl.when(k > 0)
        def _():
            project(k)

        @pl.when(outer)
        def _():
            near_copy(k, True).start()
            near_copy(k, False).start()

    def mix(k):
        near_copy(k, True).wait_recv()
        r = hid_rows(1 - own_seq)
        both = own_part[k, r, : 2 * main].astype(jnp.float32) + near_part[
            k, r, : 2 * main
        ].astype(jnp.float32)
        far_send[k, :, : 2 * main] = both.astype(jnp.bfloat16)
        tile = own_part[k, r, 2 * main :].astype(jnp.float32) + near_part[k, r, 2 * main :].astype(
            jnp.float32
        )
        far_send[k, :, 2 * main :] = put_squares(tile, get_squares(tile)).astype(jnp.bfloat16)
        far_copy(k).start()

    def act(k):
        layer = k // chunks
        near_copy(k, False).wait_recv()
        far_copy(k).wait_recv()
        r = hid_rows(own_seq)

        def total(start, stop):
            return (
                own_part[k, r, start:stop].astype(jnp.float32)
                + near_part[k, r, start:stop].astype(jnp.float32)
                + far_part[k, :, start:stop].astype(jnp.float32)
            )

        tile = total(2 * main, total_cols)
        inverse_rms = lax.rsqrt(get_squares(tile) / (width * ra) + eps)

        @pl.when(k % chunks == 0)
        def _():
            conv_pad[0:8, :] = jnp.zeros((8, conv_pad.shape[1]), jnp.float32)

        def piece(gate, up, start, stop):
            def param(row):
                return params[layer, row : row + 1, start:stop]

            conv_pad[8 : 8 + step, start:stop] = gate * inverse_rms * param(0)
            conv = param(2)
            taps = conv_weight.shape[0]
            for j in range(taps):
                first = 8 - (taps - 1) + j
                conv = conv + param(3 + j) * conv_pad[first : first + step, start:stop]
            conv_pad[0:8, start:stop] = conv_pad[step : step + 8, start:stop]
            value = conv / (1.0 + jnp.exp(-conv)) * (up * inverse_rms * param(1))
            hidden[k, r, start:stop] = value.astype(jnp.bfloat16)

        cols = 256
        for start in range(0, main, cols):
            stop = min(start + cols, main)
            piece(total(start, stop), total(main + start, main + stop), start, stop)
        if rem:
            piece(tile, pltpu.roll(tile, LANES - rem, axis=1), main, main + LANES)
        for d in (2, 1, 3):
            hid_copy(k, d, own_seq).start()

    def down(k):
        layer = k // chunks
        for seq in range(sequences):

            @pl.when(jnp.logical_not(jnp.logical_and(inner, own_seq == seq)))
            def _():
                hid_copy(k, 1, seq).wait_recv()

        value = jnp.dot(hidden[k], out_w[layer], preferred_element_type=jnp.float32)
        pair_send[k] = value[:, :half].astype(jnp.bfloat16)
        down_keep[k] = value[:, half:]
        pair_copy(k).start()

    def pair(k):
        pair_copy(k).wait_recv()
        chip_part[k, chip] = (down_keep[k] + pair_recv[k].astype(jnp.float32)).astype(jnp.bfloat16)
        for d in range(1, chips):
            chip_copy(k, d).start()

    def fold(k):
        layer = k // chunks
        for d in range(1, chips):
            chip_wait(k, d).wait_recv()
        total = chip_part[k, 0].astype(jnp.float32)
        for g in range(1, chips):
            total = total + chip_part[k, g].astype(jnp.float32)
        kept = residual_keep * state[k, :, my_cols].astype(jnp.float32)
        scale = down_scale[pl.ds(layer, 1), my_cols]
        state[k + chunks, :, my_cols] = (kept + total * scale).astype(jnp.bfloat16)
        out_copy(k, my_cols).start()

    def done(k):
        out_copy(k, other_cols).wait_recv()

        @pl.when(k >= chunks)
        def _():
            for s in range(sequences):
                c = pl.ds(pl.multiple_of((k - chunks) * step, step), step)
                out[s, c, :] = state[k + chunks, s * step : (s + 1) * step, :]

    smalls[0].wait()
    convert_in(0)
    for part in range(2):
        load(0, 2, part).start()
    for kind in range(3):
        for part in range(2):
            load(1, kind, part).start()
    project(0)
    pl.semaphore_wait(barrier, jnp.where(inner, ra - 1, ra - 2) + chips)

    works = dict(
        enter=enter, mix=mix, act=act, down=down, pair=pair, fold=fold, done=done
    )

    def prepare():
        for copy in smalls[1:]:
            copy.wait()
        for layer in range(layers):
            lines = [gate_scale[layer : layer + 1, :], up_scale[layer : layer + 1, :]]
            lines.append(conv_bias[layer : layer + 1, :])
            lines += [conv_weight[j, layer : layer + 1, :] for j in range(conv_weight.shape[0])]
            for row, line in enumerate(lines):
                if rem:
                    zeros = jnp.zeros((1, LANES - rem), jnp.float32)
                    params[layer, row : row + 1, main:] = jnp.concatenate(
                        [line[:, main:], zeros], axis=1
                    )
                params[layer, row : row + 1, :main] = line[:, :main]

    @pl.loop(0, items + max(lag for _, lag in PLAN))
    def _(slot):
        for name, lag in PLAN:
            item = slot - lag
            good = jnp.logical_and(item >= 0, item < items)
            if name in ("mix", "act"):
                good = jnp.logical_and(good, inner)

            @pl.when(good)
            def _():
                works[name](item)

            if name == "enter":

                @pl.when(slot == 0)
                def _():
                    prepare()

                for at, (kind, layer) in CONVERT.items():

                    @pl.when(slot == at)
                    def _():
                        (convert_in if kind == "in" else convert_out)(layer)

    @pl.loop(0, items)
    def _(k):
        @pl.when(outer)
        def _():
            near_copy(k, True).wait_send()
            near_copy(k, False).wait_send()

        @pl.when(inner)
        def _():
            far_copy(k).wait_send()
            for d in range(1, ra):
                hid_copy(k, d, own_seq).wait_send()

        pair_copy(k).wait_send()
        for d in range(1, chips):
            chip_copy(k, d).wait_send()
        out_copy(k, my_cols).wait_send()


def fused_shards(ra, cb, chunks, *operands):
    tokens, gate_weight = operands[0], operands[2]
    layers = 2
    sequences, length, width = tokens.shape
    units = gate_weight.shape[2]
    main = units // LANES * LANES
    total_cols = 2 * main + LANES
    padded = main + (LANES if units > main else 0)
    step = length // chunks
    rows = sequences * step
    items = layers * chunks
    half = width // 2
    chips = cb // 2
    taps = operands[6].shape[1]
    hbm = pl.BlockSpec(memory_space=pl.ANY)
    dma = pltpu.SemaphoreType.DMA
    bf16, f32 = jnp.bfloat16, jnp.float32
    return pl.pallas_call(
        functools.partial(fused, chunks, ra, cb),
        out_shape=pltpu.VMEM(tokens.shape, tokens.dtype),
        in_specs=[hbm] * 10,
        out_specs=pl.BlockSpec(memory_space=pltpu.VMEM),
        scratch_shapes=[
            pltpu.VMEM((layers, units, width), f32),
            pltpu.VMEM((layers, units, width), f32),
            pltpu.VMEM((layers, units, width), f32),
            pltpu.VMEM((layers, width), f32),
            pltpu.VMEM((layers, units), f32),
            pltpu.VMEM((layers, units), f32),
            pltpu.VMEM((taps, layers, units), f32),
            pltpu.VMEM((layers, units), f32),
            pltpu.VMEM((layers, width), f32),
            pltpu.VMEM((layers, total_cols, width), bf16),
            pltpu.VMEM((layers, padded, width), bf16),
            pltpu.VMEM((items + chunks, rows, width), bf16),
            pltpu.VMEM((items, rows, total_cols), bf16),
            pltpu.VMEM((items, rows, total_cols), bf16),
            pltpu.VMEM((items, step, total_cols), bf16),
            pltpu.VMEM((items, step, total_cols), bf16),
            pltpu.VMEM((items, rows, padded), bf16),
            pltpu.VMEM((items, rows, half), f32),
            pltpu.VMEM((items, rows, half), bf16),
            pltpu.VMEM((items, rows, half), bf16),
            pltpu.VMEM((items, chips, rows, half), bf16),
            pltpu.VMEM((8 + step, padded), f32),
            pltpu.VMEM((layers, 3 + taps, padded), f32),
            dma((layers * 6,)),
            dma((6,)),
            dma((chunks, sequences)),
            dma((items, sequences)),
            dma((items, sequences)),
            dma((items,)),
            dma((items,)),
            dma((items, ra - 1)),
            dma((items, sequences)),
            dma((items,)),
            dma((items,)),
            dma((items, chips - 1)),
            dma((items, chips - 1)),
            dma((items,)),
            dma((items,)),
        ],
        compiler_params=pltpu.CompilerParams(
            collective_id=0, has_side_effects=True, vmem_limit_bytes=60 * 1024 * 1024
        ),
    )(
        *operands[:2],
        jnp.swapaxes(gate_weight, 1, 2),
        operands[3],
        jnp.swapaxes(operands[4], 1, 2),
        operands[5],
        jnp.swapaxes(operands[6], 0, 1),
        *operands[7:],
    )


def fits(ra, cb, chunks, shape, local_width, local_units):
    rem = local_units % LANES
    return (
        ra == 4
        and cb % 2 == 0
        and cb >= 4
        and shape[0] == 2
        and shape[1] % (chunks * 16) == 0
        and local_width % (2 * LANES) == 0
        and local_units % 32 == 0
        and 2 * rem + 2 <= LANES
        and local_units >= 2 * LANES
    )


def either(ra, cb, *operands):
    tokens, gate_weight = operands[0], operands[2]
    if fits(ra, cb, CHUNKS, tokens.shape, tokens.shape[2], gate_weight.shape[2]):
        return fused_shards(ra, cb, CHUNKS, *operands)
    return shards(*operands)


def solution(mesh):
    in_specs = (
        P(None, None, "ra"),
        P(None, "ra"),
        P(None, "ra", "cb"),
        P(None, "cb"),
        P(None, "ra", "cb"),
        P(None, "cb"),
        P(None, None, "cb"),
        P(None, "cb"),
        P(None, "cb", "ra"),
        P(None, "ra"),
    )
    out_specs = P(None, None, "ra")
    return jax.shard_map(
        functools.partial(either, mesh.shape["ra"], mesh.shape["cb"]),
        mesh=mesh,
        in_specs=in_specs,
        out_specs=out_specs,
        check_vma=False,
    )
```

```python
import functools

import jax
import jax.numpy as jnp
from jax import lax
from jax.experimental import pallas as pl
from jax.experimental.pallas import tpu as pltpu
from jax.sharding import PartitionSpec as P

eps = 1e-06
residual_keep = 0.5


def causal_mix(gate_seq, conv_taps, conv_shift):
    count = conv_taps.shape[0]
    length = gate_seq.shape[1]
    padded = jnp.pad(gate_seq, ((0, 0), (count - 1, 0), (0, 0)))
    running = jnp.zeros_like(gate_seq) + conv_shift[None, None, :]
    for offset in range(count):
        running = (
            running + conv_taps[offset][None, None, :] * padded[:, offset : offset + length, :]
        )
    return running


def sublayer(current, norm_g, gate_w, gate_s, up_w, up_s, conv_taps, conv_shift, down_w, down_s):
    sequences, length, local_width = current.shape
    row_count = sequences * length
    values = current.astype(jnp.float32).reshape(row_count, local_width)
    squares = jnp.sum(values * values, axis=1)
    scaled = (values * norm_g[None, :]).astype(jnp.bfloat16)
    gate_part = jnp.dot(scaled, gate_w.astype(jnp.bfloat16), preferred_element_type=jnp.float32)
    up_part = jnp.dot(scaled, up_w.astype(jnp.bfloat16), preferred_element_type=jnp.float32)
    gate_sum, up_sum = (
        lax.psum_scatter(gate_part, "ra", scatter_dimension=1, tiled=True),
        lax.psum_scatter(up_part, "ra", scatter_dimension=1, tiled=True),
    )
    square_sum = lax.psum(squares, "ra")
    share_cols = gate_sum.shape[1]
    col_start = lax.axis_index("ra") * share_cols
    col_gate = lax.dynamic_slice_in_dim(gate_s, col_start, share_cols, 0)
    col_up = lax.dynamic_slice_in_dim(up_s, col_start, share_cols, 0)
    used_taps = lax.dynamic_slice_in_dim(conv_taps, col_start, share_cols, 1)
    used_shift = lax.dynamic_slice_in_dim(conv_shift, col_start, share_cols, 0)
    inverse_rms = lax.rsqrt(square_sum / (local_width * lax.axis_size("ra")) + eps)[:, None]
    gate_sum = gate_sum * inverse_rms * col_gate[None, :]
    up_sum = up_sum * inverse_rms * col_up[None, :]
    units = gate_sum.shape[1]
    conv_out = causal_mix(gate_sum.reshape(sequences, length, units), used_taps, used_shift)
    hidden_act = (jax.nn.silu(conv_out) * up_sum.reshape(sequences, length, units)).astype(
        jnp.bfloat16
    )
    hidden_act = hidden_act.reshape(row_count, units)
    hidden_act = lax.all_gather(hidden_act, "ra", axis=1, tiled=True)
    down_part = jnp.dot(hidden_act, down_w.astype(jnp.bfloat16), preferred_element_type=jnp.float32)
    down_sum = lax.psum(down_part, "cb")
    branch = down_sum * down_s[None, :]
    return (
        (residual_keep * values + branch)
        .astype(jnp.bfloat16)
        .reshape(sequences, length, local_width)
    )


def shards(
    tokens,
    norm_gain,
    gate_weight,
    gate_scale,
    up_weight,
    up_scale,
    conv_weight,
    conv_bias,
    down_weight,
    down_scale,
):
    current = tokens
    for layer_index in range(2):
        current = sublayer(
            current,
            norm_gain[layer_index],
            gate_weight[layer_index],
            gate_scale[layer_index],
            up_weight[layer_index],
            up_scale[layer_index],
            conv_weight[layer_index],
            conv_bias[layer_index],
            down_weight[layer_index],
            down_scale[layer_index],
        )
    return current


MESH = pl.DeviceIdType.MESH
LANES = 128
CHUNKS = 8
GROUPS = 2
PLAN = (('done', 8), ('act', 3), ('enter', 0), ('pair', 5), ('fold', 7), ('mix', 1), ('down', 4))
CONVERT = {1: ("out", 0), 3: ("in", 1), 5: ("out", 1)}


def fused(
    chunks,
    ra,
    cb,
    tokens_hbm,
    norm_gain_hbm,
    gate_weight,
    gate_scale_hbm,
    up_weight,
    up_scale_hbm,
    conv_weight_hbm,
    conv_bias_hbm,
    down_weight,
    down_scale_hbm,
    out,
    stage_gate,
    stage_up,
    stage_down,
    norm_gain,
    gate_scale,
    up_scale,
    conv_weight,
    conv_bias,
    down_scale,
    in_w,
    out_w,
    state,
    own_part,
    near_part,
    far_send,
    far_part,
    hidden,
    down_keep,
    pair_send,
    pair_recv,
    chip_part,
    conv_pad,
    params,
    load_sem,
    small_sem,
    token_sem,
    near_s,
    near_r,
    far_s,
    far_r,
    hid_s,
    hid_r,
    pair_s,
    pair_r,
    chip_s,
    chip_r,
    out_s,
    out_r,
):
    layers = 2
    sequences, length, width = tokens_hbm.shape
    units = gate_weight.shape[1]
    main = units // LANES * LANES
    rem = units - main
    total_cols = 2 * main + LANES
    step = length // chunks
    rows = sequences * step
    items = layers * chunks
    half = width // 2
    chips = cb // 2
    size = main // GROUPS
    lines_in = [(0, 2 * size + LANES)]
    lines_hid = [(0, size + (LANES if rem else 0))]
    for g in range(1, GROUPS):
        lines_in.append((sum(lines_in[-1]), 2 * size))
        lines_hid.append((sum(lines_hid[-1]), size))
    me = lax.axis_index("ra")
    mine = lax.axis_index("cb")
    core = lax.rem(mine, 2)
    chip = mine // 2
    inner = jnp.logical_and(me >= 1, me <= 2)
    outer = jnp.logical_not(inner)
    own_seq = me - 1
    my_cols = pl.ds(pl.multiple_of(core * half, LANES), half)
    other_cols = pl.ds(pl.multiple_of((1 - core) * half, LANES), half)

    barrier = pltpu.get_barrier_semaphore()
    for d in range(1, ra):
        to = lax.rem(me + d, ra)

        @pl.when(jnp.logical_or(inner, jnp.logical_and(to >= 1, to <= 2)))
        def _():
            pl.semaphore_signal(barrier, inc=1, device_id={"ra": to}, device_id_type=MESH)

    pl.semaphore_signal(
        barrier, inc=1, device_id={"cb": 2 * chip + 1 - core}, device_id_type=MESH
    )
    for d in range(1, chips):
        pl.semaphore_signal(
            barrier,
            inc=1,
            device_id={"cb": 2 * lax.rem(chip + d, chips) + core},
            device_id_type=MESH,
        )

    def token_copy(c, s):
        return pltpu.make_async_copy(
            tokens_hbm.at[s, pl.ds(pl.multiple_of(c * step, step), step)],
            state.at[c, pl.ds(s * step, step)],
            token_sem.at[c, s],
        )

    smalls = [
        pltpu.make_async_copy(src, dst, small_sem.at[i])
        for i, (src, dst) in enumerate(
            (
                (norm_gain_hbm, norm_gain),
                (gate_scale_hbm, gate_scale),
                (up_scale_hbm, up_scale),
                (conv_weight_hbm, conv_weight),
                (conv_bias_hbm, conv_bias),
                (down_scale_hbm, down_scale),
            )
        )
    ]
    pieces = [(g * size, size) for g in range(GROUPS)] + ([(main, rem)] if rem else [])
    early = [0] + list(range(GROUPS, len(pieces))) + list(range(1, GROUPS))

    def load(layer, kind, part):
        src, dst = ((gate_weight, stage_gate), (up_weight, stage_up))[kind]
        r = pl.ds(*pieces[part])
        return pltpu.make_async_copy(
            src.at[layer, r], dst.at[layer, r], load_sem.at[layer, kind * len(pieces) + part]
        )

    def load_out(layer):
        return pltpu.make_async_copy(
            down_weight.at[layer], stage_down.at[layer], load_sem.at[layer, 2 * len(pieces)]
        )

    for s in range(sequences):
        token_copy(0, s).start()
    smalls[0].start()
    for part in early:
        for kind in range(2):
            load(0, kind, part).start()
    for copy in smalls[1:]:
        copy.start()
    for c in range(1, chunks):
        for s in range(sequences):
            token_copy(c, s).start()

    block = 32

    def convert_piece(layer, kind, part):
        load(layer, kind, part).wait()
        src = (stage_gate, stage_up)[kind]
        if part < GROUPS:
            shift = lines_in[part][0] + kind * size - part * size

            @pl.loop(part * size // block, (part + 1) * size // block)
            def _(i):
                r = pl.ds(pl.multiple_of(i * block, block), block)
                r2 = pl.ds(pl.multiple_of(shift + i * block, block), block)
                in_w[layer, r2, :] = src[layer, r, :].astype(jnp.bfloat16)

        else:
            first = 2 * size + kind * rem
            in_w[layer, first : first + rem, :] = src[layer, main:, :].astype(jnp.bfloat16)

    def convert_group(layer, g):
        for part in [g] + (list(range(GROUPS, len(pieces))) if g == 0 else []):
            for kind in range(2):
                convert_piece(layer, kind, part)
        if g == 0:
            first = 2 * size + 2 * rem
            in_w[layer, first : 2 * size + LANES, :] = jnp.zeros(
                (LANES - 2 * rem, width), jnp.bfloat16
            )

    def convert_in(layer):
        for g in range(GROUPS):
            convert_group(layer, g)

    def convert_out(layer):
        load_out(layer).wait()

        def rows_to(first, shift, count):
            @pl.loop(first // block, (first + count) // block)
            def _(i):
                r = pl.ds(pl.multiple_of(i * block, block), block)
                r2 = pl.ds(pl.multiple_of(shift + i * block, block), block)
                out_w[layer, r2, :half] = stage_down[layer, r, other_cols].astype(jnp.bfloat16)
                out_w[layer, r2, half:] = stage_down[layer, r, my_cols].astype(jnp.bfloat16)

        for g in range(GROUPS):
            rows_to(g * size, lines_hid[g][0] - g * size, size)
        if rem:
            rows_to(main, size - main, rem)
            out_w[layer, size + rem : size + LANES, :] = jnp.zeros(
                (LANES - rem, width), jnp.bfloat16
            )

    lane = lax.broadcasted_iota(jnp.int32, (1, LANES), 1)

    def put_squares(tile, squares):
        high = squares.astype(jnp.bfloat16).astype(jnp.float32)
        low = squares - high
        return jnp.where(lane == 2 * rem, high, jnp.where(lane == 2 * rem + 1, low, tile))

    def get_squares(tile):
        keep = jnp.logical_and(lane >= 2 * rem, lane < 2 * rem + 2)
        return jnp.sum(jnp.where(keep, tile, 0.0), axis=1, keepdims=True)

    def near_copy(k, first, g):
        to = jnp.where(me == 0, 1, 2)
        passed = jnp.where(me < 2, 1, 0)
        r = hid_rows(passed if first else 1 - passed)
        return pltpu.make_async_remote_copy(
            src_ref=own_part.at[k, r, pl.ds(*lines_in[g])],
            dst_ref=near_part.at[k, r, pl.ds(*lines_in[g])],
            send_sem=near_s.at[k, 2 * g + int(first)],
            recv_sem=near_r.at[k, 2 * g + int(first)],
            device_id={"ra": to},
            device_id_type=MESH,
        )

    def far_copy(k, g):
        return pltpu.make_async_remote_copy(
            src_ref=far_send.at[k, :, pl.ds(*lines_in[g])],
            dst_ref=far_part.at[k, :, pl.ds(*lines_in[g])],
            send_sem=far_s.at[k, g],
            recv_sem=far_r.at[k, g],
            device_id={"ra": 3 - me},
            device_id_type=MESH,
        )

    def hid_rows(seq):
        return pl.ds(pl.multiple_of(seq * step, step), step)

    def hid_copy(k, d, seq, g):
        return pltpu.make_async_remote_copy(
            src_ref=hidden.at[k, hid_rows(seq), pl.ds(*lines_hid[g])],
            dst_ref=hidden.at[k, hid_rows(seq), pl.ds(*lines_hid[g])],
            send_sem=hid_s.at[k, (d - 1) * GROUPS + g],
            recv_sem=hid_r.at[k, seq * GROUPS + g],
            device_id={"ra": lax.rem(me + d, ra)},
            device_id_type=MESH,
        )

    def pair_copy(k):
        return pltpu.make_async_remote_copy(
            src_ref=pair_send.at[k],
            dst_ref=pair_recv.at[k],
            send_sem=pair_s.at[k],
            recv_sem=pair_r.at[k],
            device_id={"cb": 2 * chip + 1 - core},
            device_id_type=MESH,
        )

    def chip_copy(k, d):
        return pltpu.make_async_remote_copy(
            src_ref=chip_part.at[k, chip],
            dst_ref=chip_part.at[k, chip],
            send_sem=chip_s.at[k, d - 1],
            recv_sem=chip_r.at[k, d - 1],
            device_id={"cb": 2 * lax.rem(chip + d, chips) + core},
            device_id_type=MESH,
        )

    def chip_wait(k, d):
        return pltpu.make_async_remote_copy(
            src_ref=chip_part.at[k, chip],
            dst_ref=chip_part.at[k, lax.rem(chip - d + chips, chips)],
            send_sem=chip_s.at[k, d - 1],
            recv_sem=chip_r.at[k, d - 1],
            device_id={"cb": 2 * lax.rem(chip + d, chips) + core},
            device_id_type=MESH,
        )

    def out_copy(k, cols):
        return pltpu.make_async_remote_copy(
            src_ref=state.at[k + chunks, :, cols],
            dst_ref=state.at[k + chunks, :, cols],
            send_sem=out_s.at[k],
            recv_sem=out_r.at[k],
            device_id={"cb": 2 * chip + 1 - core},
            device_id_type=MESH,
        )

    def scaled_rows(k):
        layer = k // chunks

        @pl.when(k < chunks)
        def _():
            for s in range(sequences):
                token_copy(k, s).wait()

        values = state[k].astype(jnp.float32)
        squares = jnp.sum(values * values, axis=1, keepdims=True)
        gain = norm_gain[pl.ds(layer, 1), :]
        return (values * gain).astype(jnp.bfloat16), squares

    def project(k, scaled, squares, g):
        layer = k // chunks
        begin, count = lines_in[g]
        cols = 512

        def product(start, stop):
            return lax.dot_general(
                scaled,
                in_w[layer, start:stop, :],
                (((1,), (1,)), ((), ())),
                preferred_element_type=jnp.float32,
            )

        plain = begin + 2 * size
        for start in range(begin, plain, cols):
            stop = min(start + cols, plain)
            own_part[k, :, start:stop] = product(start, stop).astype(jnp.bfloat16)
        if g == 0:
            tile = put_squares(product(plain, plain + LANES), squares)
            own_part[k, :, plain : plain + LANES] = tile.astype(jnp.bfloat16)

    def send_near(k, g, which=(True, False)):
        @pl.when(outer)
        def _():
            for first in which:
                near_copy(k, first, g).start()

    def enter(k):
        @pl.when(k > 0)
        def _():
            scaled, squares = scaled_rows(k)
            for g in range(GROUPS):
                project(k, scaled, squares, g)
                send_near(k, g, (True,))
            for g in range(GROUPS):
                send_near(k, g, (False,))

    def mix(k):
        r = hid_rows(1 - own_seq)
        for g in range(GROUPS):
            near_copy(k, True, g).wait_recv()
            begin = lines_in[g][0]
            plain = begin + 2 * size

            def both(start, stop):
                return own_part[k, r, start:stop].astype(jnp.float32) + near_part[
                    k, r, start:stop
                ].astype(jnp.float32)

            far_send[k, :, begin:plain] = both(begin, plain).astype(jnp.bfloat16)
            if g == 0:
                tile = both(plain, plain + LANES)
                far_send[k, :, plain : plain + LANES] = put_squares(
                    tile, get_squares(tile)
                ).astype(jnp.bfloat16)
            far_copy(k, g).start()

    def act(k):
        layer = k // chunks
        r = hid_rows(own_seq)

        def total(start, stop):
            return (
                own_part[k, r, start:stop].astype(jnp.float32)
                + near_part[k, r, start:stop].astype(jnp.float32)
                + far_part[k, :, start:stop].astype(jnp.float32)
            )

        @pl.when(k % chunks == 0)
        def _():
            conv_pad[0:8, :] = jnp.zeros((8, conv_pad.shape[1]), jnp.float32)

        def piece(inverse_rms, gate, up, start, stop):
            def param(row):
                return params[layer, row : row + 1, start:stop]

            conv_pad[8 : 8 + step, start:stop] = gate * inverse_rms * param(0)
            conv = param(2)
            taps = conv_weight.shape[0]
            for j in range(taps):
                first = 8 - (taps - 1) + j
                conv = conv + param(3 + j) * conv_pad[first : first + step, start:stop]
            conv_pad[0:8, start:stop] = conv_pad[step : step + 8, start:stop]
            value = conv / (1.0 + jnp.exp(-conv)) * (up * inverse_rms * param(1))
            hidden[k, r, start:stop] = value.astype(jnp.bfloat16)

        cols = 256
        inverse_rms = None
        for g in range(GROUPS):
            near_copy(k, False, g).wait_recv()
            far_copy(k, g).wait_recv()
            begin, to = lines_in[g][0], lines_hid[g][0]
            if g == 0:
                tile = total(2 * size, 2 * size + LANES)
                inverse_rms = lax.rsqrt(get_squares(tile) / (width * ra) + eps)
                if rem:
                    up = pltpu.roll(tile, LANES - rem, axis=1)
                    piece(inverse_rms, tile, up, size, size + LANES)
            for start in range(0, size, cols):
                stop = min(start + cols, size)
                gate = total(begin + start, begin + stop)
                up = total(begin + size + start, begin + size + stop)
                piece(inverse_rms, gate, up, to + start, to + stop)
            for d in (2, 1, 3):
                hid_copy(k, d, own_seq, g).start()

    def down(k):
        layer = k // chunks
        for seq in range(sequences):

            @pl.when(jnp.logical_not(jnp.logical_and(inner, own_seq == seq)))
            def _():
                for g in range(GROUPS):
                    hid_copy(k, 1, seq, g).wait_recv()

        value = jnp.dot(hidden[k], out_w[layer], preferred_element_type=jnp.float32)
        pair_send[k] = value[:, :half].astype(jnp.bfloat16)
        down_keep[k] = value[:, half:]
        pair_copy(k).start()

    def pair(k):
        pair_copy(k).wait_recv()
        chip_part[k, chip] = (down_keep[k] + pair_recv[k].astype(jnp.float32)).astype(jnp.bfloat16)
        for d in range(1, chips):
            chip_copy(k, d).start()

    def fold(k):
        layer = k // chunks
        for d in range(1, chips):
            chip_wait(k, d).wait_recv()
        total = chip_part[k, 0].astype(jnp.float32)
        for g in range(1, chips):
            total = total + chip_part[k, g].astype(jnp.float32)
        kept = residual_keep * state[k, :, my_cols].astype(jnp.float32)
        scale = down_scale[pl.ds(layer, 1), my_cols]
        state[k + chunks, :, my_cols] = (kept + total * scale).astype(jnp.bfloat16)
        out_copy(k, my_cols).start()

    def done(k):
        out_copy(k, other_cols).wait_recv()

        @pl.when(k >= chunks)
        def _():
            for s in range(sequences):
                c = pl.ds(pl.multiple_of((k - chunks) * step, step), step)
                out[s, c, :] = state[k + chunks, s * step : (s + 1) * step, :]

    smalls[0].wait()
    first_scaled, first_squares = scaled_rows(0)
    for g in range(GROUPS):
        convert_group(0, g)
        if g == GROUPS - 1:
            load_out(0).start()
            for part in early:
                for kind in range(2):
                    load(1, kind, part).start()
            load_out(1).start()
        project(0, first_scaled, first_squares, g)
        if g == 0:
            pl.semaphore_wait(barrier, jnp.where(inner, ra - 1, ra - 2) + chips)
        send_near(0, g)

    works = dict(
        enter=enter, mix=mix, act=act, down=down, pair=pair, fold=fold, done=done
    )

    def prepare():
        for copy in smalls[1:]:
            copy.wait()
        for layer in range(layers):
            lines = [gate_scale[layer : layer + 1, :], up_scale[layer : layer + 1, :]]
            lines.append(conv_bias[layer : layer + 1, :])
            lines += [conv_weight[j, layer : layer + 1, :] for j in range(conv_weight.shape[0])]
            for row, line in enumerate(lines):
                if rem:
                    zeros = jnp.zeros((1, LANES - rem), jnp.float32)
                    params[layer, row : row + 1, size : size + LANES] = jnp.concatenate(
                        [line[:, main:], zeros], axis=1
                    )
                for g in range(GROUPS):
                    to = lines_hid[g][0]
                    params[layer, row : row + 1, to : to + size] = line[
                        :, g * size : (g + 1) * size
                    ]

    @pl.loop(0, items + max(lag for _, lag in PLAN))
    def _(slot):
        for name, lag in PLAN:
            item = slot - lag
            good = jnp.logical_and(item >= 0, item < items)
            if name in ("mix", "act"):
                good = jnp.logical_and(good, inner)

            @pl.when(good)
            def _():
                works[name](item)

            if name == "enter":

                @pl.when(slot == 0)
                def _():
                    prepare()

                for at, (kind, layer) in CONVERT.items():

                    @pl.when(slot == at)
                    def _():
                        (convert_in if kind == "in" else convert_out)(layer)

    @pl.loop(0, items)
    def _(k):
        @pl.when(outer)
        def _():
            for g in range(GROUPS):
                near_copy(k, True, g).wait_send()
                near_copy(k, False, g).wait_send()

        @pl.when(inner)
        def _():
            for g in range(GROUPS):
                far_copy(k, g).wait_send()
                for d in range(1, ra):
                    hid_copy(k, d, own_seq, g).wait_send()

        pair_copy(k).wait_send()
        for d in range(1, chips):
            chip_copy(k, d).wait_send()
        out_copy(k, my_cols).wait_send()


def fused_shards(ra, cb, chunks, *operands):
    tokens, gate_weight = operands[0], operands[2]
    layers = 2
    sequences, length, width = tokens.shape
    units = gate_weight.shape[2]
    main = units // LANES * LANES
    total_cols = 2 * main + LANES
    padded = main + (LANES if units > main else 0)
    step = length // chunks
    rows = sequences * step
    items = layers * chunks
    half = width // 2
    chips = cb // 2
    taps = operands[6].shape[1]
    hbm = pl.BlockSpec(memory_space=pl.ANY)
    dma = pltpu.SemaphoreType.DMA
    bf16, f32 = jnp.bfloat16, jnp.float32
    return pl.pallas_call(
        functools.partial(fused, chunks, ra, cb),
        out_shape=pltpu.VMEM(tokens.shape, tokens.dtype),
        in_specs=[hbm] * 10,
        out_specs=pl.BlockSpec(memory_space=pltpu.VMEM),
        scratch_shapes=[
            pltpu.VMEM((layers, units, width), f32),
            pltpu.VMEM((layers, units, width), f32),
            pltpu.VMEM((layers, units, width), f32),
            pltpu.VMEM((layers, width), f32),
            pltpu.VMEM((layers, units), f32),
            pltpu.VMEM((layers, units), f32),
            pltpu.VMEM((taps, layers, units), f32),
            pltpu.VMEM((layers, units), f32),
            pltpu.VMEM((layers, width), f32),
            pltpu.VMEM((layers, total_cols, width), bf16),
            pltpu.VMEM((layers, padded, width), bf16),
            pltpu.VMEM((items + chunks, rows, width), bf16),
            pltpu.VMEM((items, rows, total_cols), bf16),
            pltpu.VMEM((items, rows, total_cols), bf16),
            pltpu.VMEM((items, step, total_cols), bf16),
            pltpu.VMEM((items, step, total_cols), bf16),
            pltpu.VMEM((items, rows, padded), bf16),
            pltpu.VMEM((items, rows, half), f32),
            pltpu.VMEM((items, rows, half), bf16),
            pltpu.VMEM((items, rows, half), bf16),
            pltpu.VMEM((items, chips, rows, half), bf16),
            pltpu.VMEM((8 + step, padded), f32),
            pltpu.VMEM((layers, 3 + taps, padded), f32),
            dma((layers, 2 * GROUPS + 3)),
            dma((6,)),
            dma((chunks, sequences)),
            dma((items, 2 * GROUPS)),
            dma((items, 2 * GROUPS)),
            dma((items, GROUPS)),
            dma((items, GROUPS)),
            dma((items, (ra - 1) * GROUPS)),
            dma((items, sequences * GROUPS)),
            dma((items,)),
            dma((items,)),
            dma((items, chips - 1)),
            dma((items, chips - 1)),
            dma((items,)),
            dma((items,)),
        ],
        compiler_params=pltpu.CompilerParams(
            collective_id=0, has_side_effects=True, vmem_limit_bytes=60 * 1024 * 1024
        ),
    )(
        *operands[:2],
        jnp.swapaxes(gate_weight, 1, 2),
        operands[3],
        jnp.swapaxes(operands[4], 1, 2),
        operands[5],
        jnp.swapaxes(operands[6], 0, 1),
        *operands[7:],
    )


def fits(ra, cb, chunks, shape, local_width, local_units):
    rem = local_units % LANES
    return (
        ra == 4
        and cb % 2 == 0
        and cb >= 4
        and shape[0] == 2
        and shape[1] % (chunks * 16) == 0
        and local_width % (2 * LANES) == 0
        and local_units % 32 == 0
        and 2 * rem + 2 <= LANES
        and local_units >= LANES * GROUPS
        and local_units // LANES % GROUPS == 0
    )


def either(ra, cb, *operands):
    tokens, gate_weight = operands[0], operands[2]
    if fits(ra, cb, CHUNKS, tokens.shape, tokens.shape[2], gate_weight.shape[2]):
        return fused_shards(ra, cb, CHUNKS, *operands)
    return shards(*operands)


def solution(mesh):
    in_specs = (
        P(None, None, "ra"),
        P(None, "ra"),
        P(None, "ra", "cb"),
        P(None, "cb"),
        P(None, "ra", "cb"),
        P(None, "cb"),
        P(None, None, "cb"),
        P(None, "cb"),
        P(None, "cb", "ra"),
        P(None, "ra"),
    )
    out_specs = P(None, None, "ra")
    return jax.shard_map(
        functools.partial(either, mesh.shape["ra"], mesh.shape["cb"]),
        mesh=mesh,
        in_specs=in_specs,
        out_specs=out_specs,
        check_vma=False,
    )
```

```python
import functools

import jax
import jax.numpy as jnp
from jax import lax
from jax.experimental import pallas as pl
from jax.experimental.pallas import tpu as pltpu
from jax.sharding import PartitionSpec as P

eps = 1e-06
residual_keep = 0.5


def causal_mix(gate_seq, conv_taps, conv_shift):
    count = conv_taps.shape[0]
    length = gate_seq.shape[1]
    padded = jnp.pad(gate_seq, ((0, 0), (count - 1, 0), (0, 0)))
    running = jnp.zeros_like(gate_seq) + conv_shift[None, None, :]
    for offset in range(count):
        running = (
            running + conv_taps[offset][None, None, :] * padded[:, offset : offset + length, :]
        )
    return running


def sublayer(current, norm_g, gate_w, gate_s, up_w, up_s, conv_taps, conv_shift, down_w, down_s):
    sequences, length, local_width = current.shape
    row_count = sequences * length
    values = current.astype(jnp.float32).reshape(row_count, local_width)
    squares = jnp.sum(values * values, axis=1)
    scaled = (values * norm_g[None, :]).astype(jnp.bfloat16)
    gate_part = jnp.dot(scaled, gate_w.astype(jnp.bfloat16), preferred_element_type=jnp.float32)
    up_part = jnp.dot(scaled, up_w.astype(jnp.bfloat16), preferred_element_type=jnp.float32)
    gate_sum, up_sum = (
        lax.psum_scatter(gate_part, "ra", scatter_dimension=1, tiled=True),
        lax.psum_scatter(up_part, "ra", scatter_dimension=1, tiled=True),
    )
    square_sum = lax.psum(squares, "ra")
    share_cols = gate_sum.shape[1]
    col_start = lax.axis_index("ra") * share_cols
    col_gate = lax.dynamic_slice_in_dim(gate_s, col_start, share_cols, 0)
    col_up = lax.dynamic_slice_in_dim(up_s, col_start, share_cols, 0)
    used_taps = lax.dynamic_slice_in_dim(conv_taps, col_start, share_cols, 1)
    used_shift = lax.dynamic_slice_in_dim(conv_shift, col_start, share_cols, 0)
    inverse_rms = lax.rsqrt(square_sum / (local_width * lax.axis_size("ra")) + eps)[:, None]
    gate_sum = gate_sum * inverse_rms * col_gate[None, :]
    up_sum = up_sum * inverse_rms * col_up[None, :]
    units = gate_sum.shape[1]
    conv_out = causal_mix(gate_sum.reshape(sequences, length, units), used_taps, used_shift)
    hidden_act = (jax.nn.silu(conv_out) * up_sum.reshape(sequences, length, units)).astype(
        jnp.bfloat16
    )
    hidden_act = hidden_act.reshape(row_count, units)
    hidden_act = lax.all_gather(hidden_act, "ra", axis=1, tiled=True)
    down_part = jnp.dot(hidden_act, down_w.astype(jnp.bfloat16), preferred_element_type=jnp.float32)
    down_sum = lax.psum(down_part, "cb")
    branch = down_sum * down_s[None, :]
    return (
        (residual_keep * values + branch)
        .astype(jnp.bfloat16)
        .reshape(sequences, length, local_width)
    )


def shards(
    tokens,
    norm_gain,
    gate_weight,
    gate_scale,
    up_weight,
    up_scale,
    conv_weight,
    conv_bias,
    down_weight,
    down_scale,
):
    current = tokens
    for layer_index in range(2):
        current = sublayer(
            current,
            norm_gain[layer_index],
            gate_weight[layer_index],
            gate_scale[layer_index],
            up_weight[layer_index],
            up_scale[layer_index],
            conv_weight[layer_index],
            conv_bias[layer_index],
            down_weight[layer_index],
            down_scale[layer_index],
        )
    return current


MESH = pl.DeviceIdType.MESH
LANES = 128
CHUNKS = 8
GROUPS = 2
PLAN = (
    ("done", 8),
    ("act", 3),
    ("fold", 7),
    ("enter", 0),
    ("mix", 1),
    ("pair", 5),
    ("down", 4),
)
WINDOW = dict(near=6, far=5, hid=6, pair=5, chip=8, out=4)
CONVERT = {1: ("out", 0), 3: ("in", 1), 5: ("out", 1)}


def fused(
    chunks,
    ra,
    cb,
    tokens_hbm,
    norm_gain_hbm,
    gate_weight,
    gate_scale_hbm,
    up_weight,
    up_scale_hbm,
    conv_weight_hbm,
    conv_bias_hbm,
    down_weight,
    down_scale_hbm,
    out,
    stage_gate,
    stage_up,
    stage_down,
    norm_gain,
    gate_scale,
    up_scale,
    conv_weight,
    conv_bias,
    down_scale,
    in_w,
    out_w,
    state,
    own_part,
    near_part,
    far_send,
    far_part,
    hidden,
    hid_rem,
    down_keep,
    pair_send,
    pair_recv,
    chip_part,
    rows_of,
    conv_pad,
    params,
    load_sem,
    small_sem,
    token_sem,
    near_s,
    near_r,
    far_s,
    far_r,
    hid_s,
    hid_r,
    rem_s,
    rem_r,
    pair_s,
    pair_r,
    chip_s,
    chip_r,
    out_s,
    out_r,
):
    layers = 2
    sequences, _, step, width = tokens_hbm.shape
    units = gate_weight.shape[1]
    main = units // LANES * LANES
    rem = units - main
    total_cols = 2 * main + LANES
    rows = sequences * step
    items = layers * chunks
    half = width // 2
    chips = cb // 2
    size = main // GROUPS
    lines_in = [(0, 2 * size + LANES)]
    lines_hid = [(0, size)]
    for g in range(1, GROUPS):
        lines_in.append((sum(lines_in[-1]), 2 * size))
        lines_hid.append((g * size + (LANES if rem else 0), size))
    me = lax.axis_index("ra")
    mine = lax.axis_index("cb")
    core = lax.rem(mine, 2)
    chip = mine // 2
    inner = jnp.logical_and(me >= 1, me <= 2)
    outer = jnp.logical_not(inner)
    own_seq = me - 1
    my_cols = pl.ds(pl.multiple_of(core * half, LANES), half)
    other_cols = pl.ds(pl.multiple_of((1 - core) * half, LANES), half)

    barrier = pltpu.get_barrier_semaphore()
    for d in range(1, ra):
        to = lax.rem(me + d, ra)

        @pl.when(jnp.logical_or(inner, jnp.logical_and(to >= 1, to <= 2)))
        def _():
            pl.semaphore_signal(barrier, inc=1, device_id={"ra": to}, device_id_type=MESH)

    pl.semaphore_signal(
        barrier, inc=1, device_id={"cb": 2 * chip + 1 - core}, device_id_type=MESH
    )
    for d in range(1, chips):
        pl.semaphore_signal(
            barrier,
            inc=1,
            device_id={"cb": 2 * lax.rem(chip + d, chips) + core},
            device_id_type=MESH,
        )

    def token_copy(s):
        return pltpu.make_async_copy(
            tokens_hbm.at[s],
            state.at[pl.ds(0, chunks), pl.ds(s * step, step)],
            token_sem.at[s],
        )

    smalls = [
        pltpu.make_async_copy(src, dst, small_sem.at[i])
        for i, (src, dst) in enumerate(
            (
                (norm_gain_hbm, norm_gain),
                (gate_scale_hbm, gate_scale),
                (up_scale_hbm, up_scale),
                (conv_weight_hbm, conv_weight),
                (conv_bias_hbm, conv_bias),
                (down_scale_hbm, down_scale),
            )
        )
    ]
    pieces = [(g * size, size) for g in range(GROUPS)] + ([(main, rem)] if rem else [])
    early = [0] + list(range(GROUPS, len(pieces))) + list(range(1, GROUPS))

    def load(layer, kind, part):
        src, dst = ((gate_weight, stage_gate), (up_weight, stage_up))[kind]
        r = pl.ds(*pieces[part])
        return pltpu.make_async_copy(
            src.at[layer, r], dst.at[layer, r], load_sem.at[layer, kind * len(pieces) + part]
        )

    def load_out(layer):
        return pltpu.make_async_copy(
            down_weight.at[layer], stage_down.at[layer], load_sem.at[layer, 2 * len(pieces)]
        )

    for s in range(sequences):
        token_copy(s).start()
    smalls[0].start()
    for part in early:
        for kind in range(2):
            load(0, kind, part).start()
    for copy in smalls[1:]:
        copy.start()

    block = 32

    def convert_piece(layer, kind, part):
        load(layer, kind, part).wait()
        src = (stage_gate, stage_up)[kind]
        if part < GROUPS:
            shift = lines_in[part][0] + kind * size - part * size

            @pl.loop(part * size // block, (part + 1) * size // block)
            def _(i):
                r = pl.ds(pl.multiple_of(i * block, block), block)
                r2 = pl.ds(pl.multiple_of(shift + i * block, block), block)
                in_w[layer, r2, :] = src[layer, r, :].astype(jnp.bfloat16)

        else:
            first = 2 * size + kind * rem
            in_w[layer, first : first + rem, :] = src[layer, main:, :].astype(jnp.bfloat16)

    def convert_group(layer, g):
        for part in [g] + (list(range(GROUPS, len(pieces))) if g == 0 else []):
            for kind in range(2):
                convert_piece(layer, kind, part)
        if g == 0:
            first = 2 * size + 2 * rem
            in_w[layer, first : 2 * size + LANES, :] = jnp.zeros(
                (LANES - 2 * rem, width), jnp.bfloat16
            )

    def convert_in(layer):
        for g in range(GROUPS):
            convert_group(layer, g)

    def convert_out(layer):
        load_out(layer).wait()

        def rows_to(first, shift, count):
            @pl.loop(first // block, (first + count) // block)
            def _(i):
                r = pl.ds(pl.multiple_of(i * block, block), block)
                r2 = pl.ds(pl.multiple_of(shift + i * block, block), block)
                out_w[layer, r2, :half] = stage_down[layer, r, other_cols].astype(jnp.bfloat16)
                out_w[layer, r2, half:] = stage_down[layer, r, my_cols].astype(jnp.bfloat16)

        for g in range(GROUPS):
            rows_to(g * size, lines_hid[g][0] - g * size, size)
        if rem:
            rows_to(main, size - main, rem)
            out_w[layer, size + rem : size + LANES, :] = jnp.zeros(
                (LANES - rem, width), jnp.bfloat16
            )

    lane = lax.broadcasted_iota(jnp.int32, (1, LANES), 1)

    def put_squares(tile, squares):
        high = squares.astype(jnp.bfloat16).astype(jnp.float32)
        low = squares - high
        return jnp.where(lane == 2 * rem, high, jnp.where(lane == 2 * rem + 1, low, tile))

    def get_squares(tile):
        keep = jnp.logical_and(lane >= 2 * rem, lane < 2 * rem + 2)
        return jnp.sum(jnp.where(keep, tile, 0.0), axis=1, keepdims=True)

    def slot_of(k, kind):
        return k % WINDOW[kind] if isinstance(k, int) else lax.rem(k, WINDOW[kind])

    def launch(k, kind, copies):
        if not isinstance(k, int):

            @pl.when(k >= WINDOW[kind])
            def _():
                for copy in copies:
                    copy.wait_send()

        for copy in copies:
            copy.start()

    def near_copy(k, first, g):
        to = jnp.where(me == 0, 1, 2)
        passed = jnp.where(me < 2, 1, 0)
        r = hid_rows(passed if first else 1 - passed)
        return pltpu.make_async_remote_copy(
            src_ref=own_part.at[k, r, pl.ds(*lines_in[g])],
            dst_ref=near_part.at[k, r, pl.ds(*lines_in[g])],
            send_sem=near_s.at[slot_of(k, "near"), 2 * g + int(first)],
            recv_sem=near_r.at[slot_of(k, "near"), 2 * g + int(first)],
            device_id={"ra": to},
            device_id_type=MESH,
        )

    def far_copy(k, g):
        return pltpu.make_async_remote_copy(
            src_ref=far_send.at[k, :, pl.ds(*lines_in[g])],
            dst_ref=far_part.at[k, :, pl.ds(*lines_in[g])],
            send_sem=far_s.at[slot_of(k, "far"), g],
            recv_sem=far_r.at[slot_of(k, "far"), g],
            device_id={"ra": 3 - me},
            device_id_type=MESH,
        )

    def hid_rows(seq):
        return pl.ds(pl.multiple_of(seq * step, step), step)

    def hid_copy(k, d, seq, g):
        return pltpu.make_async_remote_copy(
            src_ref=hidden.at[k, hid_rows(seq), pl.ds(*lines_hid[g])],
            dst_ref=hidden.at[k, hid_rows(seq), pl.ds(*lines_hid[g])],
            send_sem=hid_s.at[slot_of(k, "hid"), (d - 1) * GROUPS + g],
            recv_sem=hid_r.at[slot_of(k, "hid"), seq * GROUPS + g],
            device_id={"ra": lax.rem(me + d, ra)},
            device_id_type=MESH,
        )

    def rem_copy(k, d, seq):
        return pltpu.make_async_remote_copy(
            src_ref=hid_rem.at[k, seq],
            dst_ref=hid_rem.at[k, seq],
            send_sem=rem_s.at[slot_of(k, "hid"), d - 1],
            recv_sem=rem_r.at[slot_of(k, "hid"), seq],
            device_id={"ra": lax.rem(me + d, ra)},
            device_id_type=MESH,
        )

    def pair_copy(k):
        return pltpu.make_async_remote_copy(
            src_ref=pair_send.at[k],
            dst_ref=pair_recv.at[k],
            send_sem=pair_s.at[slot_of(k, "pair")],
            recv_sem=pair_r.at[slot_of(k, "pair")],
            device_id={"cb": 2 * chip + 1 - core},
            device_id_type=MESH,
        )

    def chip_copy(k, d):
        return pltpu.make_async_remote_copy(
            src_ref=chip_part.at[k, chip],
            dst_ref=chip_part.at[k, chip],
            send_sem=chip_s.at[slot_of(k, "chip"), d - 1],
            recv_sem=chip_r.at[slot_of(k, "chip"), d - 1],
            device_id={"cb": 2 * lax.rem(chip + d, chips) + core},
            device_id_type=MESH,
        )

    def chip_wait(k, d):
        return pltpu.make_async_remote_copy(
            src_ref=chip_part.at[k, chip],
            dst_ref=chip_part.at[k, lax.rem(chip - d + chips, chips)],
            send_sem=chip_s.at[slot_of(k, "chip"), d - 1],
            recv_sem=chip_r.at[slot_of(k, "chip"), d - 1],
            device_id={"cb": 2 * lax.rem(chip + d, chips) + core},
            device_id_type=MESH,
        )

    def out_copy(k, cols):
        return pltpu.make_async_remote_copy(
            src_ref=state.at[k + chunks, :, cols],
            dst_ref=state.at[k + chunks, :, cols],
            send_sem=out_s.at[slot_of(k, "out")],
            recv_sem=out_r.at[slot_of(k, "out")],
            device_id={"cb": 2 * chip + 1 - core},
            device_id_type=MESH,
        )

    def scaled_rows(k):
        layer = k // chunks

        values = state[k].astype(jnp.float32)
        squares = jnp.sum(values * values, axis=1, keepdims=True)
        gain = norm_gain[pl.ds(layer, 1), :]
        return (values * gain).astype(jnp.bfloat16), squares

    def project(k, scaled, squares, g):
        layer = k // chunks
        begin, count = lines_in[g]
        cols = 512

        def product(start, stop):
            return lax.dot_general(
                scaled,
                in_w[layer, start:stop, :],
                (((1,), (1,)), ((), ())),
                preferred_element_type=jnp.float32,
            )

        plain = begin + 2 * size
        for start in range(begin, plain, cols):
            stop = min(start + cols, plain)
            own_part[k, :, start:stop] = product(start, stop).astype(jnp.bfloat16)
        if g == 0:
            tile = put_squares(product(plain, plain + LANES), squares)
            own_part[k, :, plain : plain + LANES] = tile.astype(jnp.bfloat16)

    def send_near(k, g, which=(True, False)):
        @pl.when(outer)
        def _():
            launch(k, "near", [near_copy(k, first, g) for first in which])

    def enter(k):
        @pl.when(k > 0)
        def _():
            scaled, squares = scaled_rows(k)
            for g in range(GROUPS):
                project(k, scaled, squares, g)
                send_near(k, g, (True,))
            for g in range(GROUPS):
                send_near(k, g, (False,))

    def mix(k):
        r = hid_rows(1 - own_seq)
        for g in range(GROUPS):
            near_copy(k, True, g).wait_recv()
            begin = lines_in[g][0]
            plain = begin + 2 * size

            def both(start, stop):
                return own_part[k, r, start:stop].astype(jnp.float32) + near_part[
                    k, r, start:stop
                ].astype(jnp.float32)

            far_send[k, :, begin:plain] = both(begin, plain).astype(jnp.bfloat16)
            if g == 0:
                tile = both(plain, plain + LANES)
                far_send[k, :, plain : plain + LANES] = put_squares(
                    tile, get_squares(tile)
                ).astype(jnp.bfloat16)
            launch(k, "far", [far_copy(k, g)])

    def act(k):
        layer = k // chunks
        r = hid_rows(own_seq)

        def total(start, stop):
            return (
                own_part[k, r, start:stop].astype(jnp.float32)
                + near_part[k, r, start:stop].astype(jnp.float32)
                + far_part[k, :, start:stop].astype(jnp.float32)
            )

        @pl.when(k % chunks == 0)
        def _():
            conv_pad[0:8, :] = jnp.zeros((8, conv_pad.shape[1]), jnp.float32)

        def piece(inverse_rms, gate, up, start, stop):
            def param(row):
                return params[layer, row : row + 1, start:stop]

            conv_pad[8 : 8 + step, start:stop] = gate * inverse_rms * param(0)
            conv = param(2)
            taps = conv_weight.shape[0]
            for j in range(taps):
                first = 8 - (taps - 1) + j
                conv = conv + param(3 + j) * conv_pad[first : first + step, start:stop]
            conv_pad[0:8, start:stop] = conv_pad[step : step + 8, start:stop]
            value = conv / (1.0 + jnp.exp(-conv)) * (up * inverse_rms * param(1))
            return value

        cols = 256
        inverse_rms = None
        for g in range(GROUPS):
            near_copy(k, False, g).wait_recv()
            far_copy(k, g).wait_recv()
            begin, to = lines_in[g][0], lines_hid[g][0]
            if g == 0:
                tile = total(2 * size, 2 * size + LANES)
                inverse_rms = lax.rsqrt(get_squares(tile) / (width * ra) + eps)
                if rem:
                    up = pltpu.roll(tile, LANES - rem, axis=1)
                    value = piece(inverse_rms, tile, up, size, size + LANES)
                    packed = value[: step // 2] + pltpu.roll(value[step // 2 :], rem, axis=1)
                    hid_rem[k, own_seq] = packed.astype(jnp.bfloat16)
            for start in range(0, size, cols):
                stop = min(start + cols, size)
                gate = total(begin + start, begin + stop)
                up = total(begin + size + start, begin + size + stop)
                value = piece(inverse_rms, gate, up, to + start, to + stop)
                hidden[k, r, to + start : to + stop] = value.astype(jnp.bfloat16)
            copies = []
            for d in (2, 1, 3):
                if rem and g == 0:
                    copies.append(rem_copy(k, d, own_seq))
                copies.append(hid_copy(k, d, own_seq, g))
            launch(k, "hid", copies)

    def down(k):
        layer = k // chunks
        for seq in range(sequences):

            @pl.when(jnp.logical_not(jnp.logical_and(inner, own_seq == seq)))
            def _():
                if rem:
                    rem_copy(k, 1, seq).wait_recv()
                for g in range(GROUPS):
                    hid_copy(k, 1, seq, g).wait_recv()

        if rem:
            for seq in range(sequences):
                packed = hid_rem[k, seq].astype(jnp.float32)
                for part in range(2):
                    first = seq * step + part * (step // 2)
                    rows_of[first : first + step // 2, :] = (
                        pltpu.roll(packed, LANES - rem, axis=1) if part else packed
                    )
            hidden[k, :, size : size + LANES] = rows_of[...].astype(jnp.bfloat16)
        value = jnp.dot(hidden[k], out_w[layer], preferred_element_type=jnp.float32)
        pair_send[k] = value[:, :half].astype(jnp.bfloat16)
        down_keep[k] = value[:, half:]
        launch(k, "pair", [pair_copy(k)])

    def pair(k):
        pair_copy(k).wait_recv()
        chip_part[k, chip] = (down_keep[k] + pair_recv[k].astype(jnp.float32)).astype(jnp.bfloat16)
        launch(k, "chip", [chip_copy(k, d) for d in range(1, chips)])

    def fold(k):
        layer = k // chunks
        for d in range(1, chips):
            chip_wait(k, d).wait_recv()
        total = chip_part[k, 0].astype(jnp.float32)
        for g in range(1, chips):
            total = total + chip_part[k, g].astype(jnp.float32)
        kept = residual_keep * state[k, :, my_cols].astype(jnp.float32)
        scale = down_scale[pl.ds(layer, 1), my_cols]
        state[k + chunks, :, my_cols] = (kept + total * scale).astype(jnp.bfloat16)
        launch(k, "out", [out_copy(k, my_cols)])

    def done(k):
        out_copy(k, other_cols).wait_recv()

        @pl.when(k >= chunks)
        def _():
            for s in range(sequences):
                c = pl.ds(pl.multiple_of((k - chunks) * step, step), step)
                out[s, c, :] = state[k + chunks, s * step : (s + 1) * step, :]

    smalls[0].wait()
    for s in range(sequences):
        token_copy(s).wait()
    first_scaled, first_squares = scaled_rows(0)
    for g in range(GROUPS):
        convert_group(0, g)
        if g == GROUPS - 1:
            load_out(0).start()
            for part in early:
                for kind in range(2):
                    load(1, kind, part).start()
            load_out(1).start()
        project(0, first_scaled, first_squares, g)
        if g == 0:
            pl.semaphore_wait(barrier, jnp.where(inner, ra - 1, ra - 2) + chips)
        send_near(0, g)

    works = dict(
        enter=enter, mix=mix, act=act, down=down, pair=pair, fold=fold, done=done
    )

    def prepare():
        for copy in smalls[1:]:
            copy.wait()
        for layer in range(layers):
            lines = [gate_scale[layer : layer + 1, :], up_scale[layer : layer + 1, :]]
            lines.append(conv_bias[layer : layer + 1, :])
            lines += [conv_weight[j, layer : layer + 1, :] for j in range(conv_weight.shape[0])]
            for row, line in enumerate(lines):
                if rem:
                    zeros = jnp.zeros((1, LANES - rem), jnp.float32)
                    params[layer, row : row + 1, size : size + LANES] = jnp.concatenate(
                        [line[:, main:], zeros], axis=1
                    )
                for g in range(GROUPS):
                    to = lines_hid[g][0]
                    params[layer, row : row + 1, to : to + size] = line[
                        :, g * size : (g + 1) * size
                    ]

    @pl.loop(0, items + max(lag for _, lag in PLAN))
    def _(slot):
        for name, lag in PLAN:
            item = slot - lag
            good = jnp.logical_and(item >= 0, item < items)
            if name in ("mix", "act"):
                good = jnp.logical_and(good, inner)

            @pl.when(good)
            def _():
                works[name](item)

            if name == "enter":

                @pl.when(slot == 0)
                def _():
                    prepare()

                for at, (kind, layer) in CONVERT.items():

                    @pl.when(slot == at)
                    def _():
                        (convert_in if kind == "in" else convert_out)(layer)

    def drain(kind, make):
        @pl.loop(max(items - WINDOW[kind], 0), items)
        def _(k):
            for copy in make(k):
                copy.wait_send()

    @pl.when(outer)
    def _():
        drain(
            "near",
            lambda k: [near_copy(k, f, g) for f in (True, False) for g in range(GROUPS)],
        )

    @pl.when(inner)
    def _():
        drain("far", lambda k: [far_copy(k, g) for g in range(GROUPS)])
        drain(
            "hid",
            lambda k: [
                hid_copy(k, d, own_seq, g) for d in range(1, ra) for g in range(GROUPS)
            ]
            + ([rem_copy(k, d, own_seq) for d in range(1, ra)] if rem else []),
        )

    drain("pair", lambda k: [pair_copy(k)])
    drain("chip", lambda k: [chip_copy(k, d) for d in range(1, chips)])
    drain("out", lambda k: [out_copy(k, my_cols)])


def fused_shards(ra, cb, chunks, *operands):
    tokens, gate_weight = operands[0], operands[2]
    layers = 2
    sequences, length, width = tokens.shape
    units = gate_weight.shape[2]
    main = units // LANES * LANES
    total_cols = 2 * main + LANES
    padded = main + (LANES if units > main else 0)
    step = length // chunks
    rows = sequences * step
    items = layers * chunks
    half = width // 2
    chips = cb // 2
    taps = operands[6].shape[1]
    hbm = pl.BlockSpec(memory_space=pl.ANY)
    dma = pltpu.SemaphoreType.DMA
    bf16, f32 = jnp.bfloat16, jnp.float32
    return pl.pallas_call(
        functools.partial(fused, chunks, ra, cb),
        out_shape=pltpu.VMEM(tokens.shape, tokens.dtype),
        in_specs=[hbm] * 10,
        out_specs=pl.BlockSpec(memory_space=pltpu.VMEM),
        scratch_shapes=[
            pltpu.VMEM((layers, units, width), f32),
            pltpu.VMEM((layers, units, width), f32),
            pltpu.VMEM((layers, units, width), f32),
            pltpu.VMEM((layers, width), f32),
            pltpu.VMEM((layers, units), f32),
            pltpu.VMEM((layers, units), f32),
            pltpu.VMEM((taps, layers, units), f32),
            pltpu.VMEM((layers, units), f32),
            pltpu.VMEM((layers, width), f32),
            pltpu.VMEM((layers, total_cols, width), bf16),
            pltpu.VMEM((layers, padded, width), bf16),
            pltpu.VMEM((items + chunks, rows, width), bf16),
            pltpu.VMEM((items, rows, total_cols), bf16),
            pltpu.VMEM((items, rows, total_cols), bf16),
            pltpu.VMEM((items, step, total_cols), bf16),
            pltpu.VMEM((items, step, total_cols), bf16),
            pltpu.VMEM((items, rows, padded), bf16),
            pltpu.VMEM((items, sequences, step // 2, LANES), bf16),
            pltpu.VMEM((items, rows, half), f32),
            pltpu.VMEM((items, rows, half), bf16),
            pltpu.VMEM((items, rows, half), bf16),
            pltpu.VMEM((items, chips, rows, half), bf16),
            pltpu.VMEM((rows, LANES), f32),
            pltpu.VMEM((8 + step, padded), f32),
            pltpu.VMEM((layers, 3 + taps, padded), f32),
            dma((layers, 2 * GROUPS + 3)),
            dma((6,)),
            dma((sequences,)),
            dma((WINDOW["near"], 2 * GROUPS)),
            dma((WINDOW["near"], 2 * GROUPS)),
            dma((WINDOW["far"], GROUPS)),
            dma((WINDOW["far"], GROUPS)),
            dma((WINDOW["hid"], (ra - 1) * GROUPS)),
            dma((WINDOW["hid"], sequences * GROUPS)),
            dma((WINDOW["hid"], ra - 1)),
            dma((WINDOW["hid"], sequences)),
            dma((WINDOW["pair"],)),
            dma((WINDOW["pair"],)),
            dma((WINDOW["chip"], chips - 1)),
            dma((WINDOW["chip"], chips - 1)),
            dma((WINDOW["out"],)),
            dma((WINDOW["out"],)),
        ],
        compiler_params=pltpu.CompilerParams(
            collective_id=0, has_side_effects=True, vmem_limit_bytes=60 * 1024 * 1024
        ),
    )(
        tokens.reshape(sequences, chunks, step, width),
        operands[1],
        jnp.swapaxes(gate_weight, 1, 2),
        operands[3],
        jnp.swapaxes(operands[4], 1, 2),
        operands[5],
        jnp.swapaxes(operands[6], 0, 1),
        *operands[7:],
    )


def fits(ra, cb, chunks, shape, local_width, local_units):
    rem = local_units % LANES
    return (
        ra == 4
        and cb % 2 == 0
        and cb >= 4
        and shape[0] == 2
        and shape[1] % (chunks * 16) == 0
        and local_width % (2 * LANES) == 0
        and local_units % 32 == 0
        and 2 * rem + 2 <= LANES
        and local_units >= LANES * GROUPS
        and local_units // LANES % GROUPS == 0
    )


def either(ra, cb, *operands):
    tokens, gate_weight = operands[0], operands[2]
    if fits(ra, cb, CHUNKS, tokens.shape, tokens.shape[2], gate_weight.shape[2]):
        return fused_shards(ra, cb, CHUNKS, *operands)
    return shards(*operands)


def solution(mesh):
    in_specs = (
        P(None, None, "ra"),
        P(None, "ra"),
        P(None, "ra", "cb"),
        P(None, "cb"),
        P(None, "ra", "cb"),
        P(None, "cb"),
        P(None, None, "cb"),
        P(None, "cb"),
        P(None, "cb", "ra"),
        P(None, "ra"),
    )
    out_specs = P(None, None, "ra")
    return jax.shard_map(
        functools.partial(either, mesh.shape["ra"], mesh.shape["cb"]),
        mesh=mesh,
        in_specs=in_specs,
        out_specs=out_specs,
        check_vma=False,
    )
```

```python
import functools

import jax
import jax.numpy as jnp
from jax import lax
from jax.experimental import pallas as pl
from jax.experimental.pallas import tpu as pltpu
from jax.sharding import PartitionSpec as P

eps = 1e-06
residual_keep = 0.5


def causal_mix(gate_seq, conv_taps, conv_shift):
    count = conv_taps.shape[0]
    length = gate_seq.shape[1]
    padded = jnp.pad(gate_seq, ((0, 0), (count - 1, 0), (0, 0)))
    running = jnp.zeros_like(gate_seq) + conv_shift[None, None, :]
    for offset in range(count):
        running = (
            running + conv_taps[offset][None, None, :] * padded[:, offset : offset + length, :]
        )
    return running


def sublayer(current, norm_g, gate_w, gate_s, up_w, up_s, conv_taps, conv_shift, down_w, down_s):
    sequences, length, local_width = current.shape
    row_count = sequences * length
    values = current.astype(jnp.float32).reshape(row_count, local_width)
    squares = jnp.sum(values * values, axis=1)
    scaled = (values * norm_g[None, :]).astype(jnp.bfloat16)
    gate_part = jnp.dot(scaled, gate_w.astype(jnp.bfloat16), preferred_element_type=jnp.float32)
    up_part = jnp.dot(scaled, up_w.astype(jnp.bfloat16), preferred_element_type=jnp.float32)
    gate_sum, up_sum = (
        lax.psum_scatter(gate_part, "ra", scatter_dimension=1, tiled=True),
        lax.psum_scatter(up_part, "ra", scatter_dimension=1, tiled=True),
    )
    square_sum = lax.psum(squares, "ra")
    share_cols = gate_sum.shape[1]
    col_start = lax.axis_index("ra") * share_cols
    col_gate = lax.dynamic_slice_in_dim(gate_s, col_start, share_cols, 0)
    col_up = lax.dynamic_slice_in_dim(up_s, col_start, share_cols, 0)
    used_taps = lax.dynamic_slice_in_dim(conv_taps, col_start, share_cols, 1)
    used_shift = lax.dynamic_slice_in_dim(conv_shift, col_start, share_cols, 0)
    inverse_rms = lax.rsqrt(square_sum / (local_width * lax.axis_size("ra")) + eps)[:, None]
    gate_sum = gate_sum * inverse_rms * col_gate[None, :]
    up_sum = up_sum * inverse_rms * col_up[None, :]
    units = gate_sum.shape[1]
    conv_out = causal_mix(gate_sum.reshape(sequences, length, units), used_taps, used_shift)
    hidden_act = (jax.nn.silu(conv_out) * up_sum.reshape(sequences, length, units)).astype(
        jnp.bfloat16
    )
    hidden_act = hidden_act.reshape(row_count, units)
    hidden_act = lax.all_gather(hidden_act, "ra", axis=1, tiled=True)
    down_part = jnp.dot(hidden_act, down_w.astype(jnp.bfloat16), preferred_element_type=jnp.float32)
    down_sum = lax.psum(down_part, "cb")
    branch = down_sum * down_s[None, :]
    return (
        (residual_keep * values + branch)
        .astype(jnp.bfloat16)
        .reshape(sequences, length, local_width)
    )


def shards(
    tokens,
    norm_gain,
    gate_weight,
    gate_scale,
    up_weight,
    up_scale,
    conv_weight,
    conv_bias,
    down_weight,
    down_scale,
):
    current = tokens
    for layer_index in range(2):
        current = sublayer(
            current,
            norm_gain[layer_index],
            gate_weight[layer_index],
            gate_scale[layer_index],
            up_weight[layer_index],
            up_scale[layer_index],
            conv_weight[layer_index],
            conv_bias[layer_index],
            down_weight[layer_index],
            down_scale[layer_index],
        )
    return current


MESH = pl.DeviceIdType.MESH
LANES = 128
CHUNKS = 8
GROUPS = 2
PLAN = (
    ("done", 8),
    ("act", 3),
    ("fold", 7),
    ("enter", 0),
    ("mix", 1),
    ("pair", 5),
    ("down", 4),
)
WINDOW = dict(near=5, far=4, hid=5, pair=4, chip=6, out=2)
CONVERT = {1: ("out", 0), 3: ("in", 1), 5: ("out", 1)}


def fused(
    chunks,
    ra,
    cb,
    tokens_hbm,
    norm_gain_hbm,
    gate_weight,
    gate_scale_hbm,
    up_weight,
    up_scale_hbm,
    conv_weight_hbm,
    conv_bias_hbm,
    down_weight,
    down_scale_hbm,
    out,
    stage_gate,
    stage_up,
    stage_down,
    norm_gain,
    gate_scale,
    up_scale,
    conv_weight,
    conv_bias,
    down_scale,
    in_w,
    out_w,
    state,
    own_part,
    near_part,
    far_send,
    far_part,
    hidden,
    hid_rem,
    down_keep,
    pair_send,
    pair_recv,
    chip_part,
    rows_of,
    conv_pad,
    params,
    load_sem,
    small_sem,
    token_sem,
    near_s,
    near_r,
    far_s,
    far_r,
    hid_s,
    hid_r,
    rem_s,
    rem_r,
    pair_s,
    pair_r,
    chip_s,
    chip_r,
    out_s,
    out_r,
):
    layers = 2
    sequences, _, step, width = tokens_hbm.shape
    units = gate_weight.shape[1]
    main = units // LANES * LANES
    rem = units - main
    total_cols = 2 * main + LANES
    rows = sequences * step
    items = layers * chunks
    half = width // 2
    chips = cb // 2
    size = main // GROUPS
    lines_in = [(0, 2 * size + LANES)]
    lines_hid = [(0, size)]
    for g in range(1, GROUPS):
        lines_in.append((sum(lines_in[-1]), 2 * size))
        lines_hid.append((g * size + (LANES if rem else 0), size))
    me = lax.axis_index("ra")
    mine = lax.axis_index("cb")
    core = lax.rem(mine, 2)
    chip = mine // 2
    inner = jnp.logical_and(me >= 1, me <= 2)
    outer = jnp.logical_not(inner)
    own_seq = me - 1
    my_cols = pl.ds(pl.multiple_of(core * half, LANES), half)
    other_cols = pl.ds(pl.multiple_of((1 - core) * half, LANES), half)

    barrier = pltpu.get_barrier_semaphore()
    for d in range(1, ra):
        to = lax.rem(me + d, ra)

        @pl.when(jnp.logical_or(inner, jnp.logical_and(to >= 1, to <= 2)))
        def _():
            pl.semaphore_signal(barrier, inc=1, device_id={"ra": to}, device_id_type=MESH)

    pl.semaphore_signal(
        barrier, inc=1, device_id={"cb": 2 * chip + 1 - core}, device_id_type=MESH
    )
    for d in range(1, chips):
        pl.semaphore_signal(
            barrier,
            inc=1,
            device_id={"cb": 2 * lax.rem(chip + d, chips) + core},
            device_id_type=MESH,
        )

    def token_copy(s):
        return pltpu.make_async_copy(
            tokens_hbm.at[s],
            state.at[pl.ds(0, chunks), pl.ds(s * step, step)],
            token_sem.at[s],
        )

    smalls = [
        pltpu.make_async_copy(src, dst, small_sem.at[i])
        for i, (src, dst) in enumerate(
            (
                (norm_gain_hbm, norm_gain),
                (gate_scale_hbm, gate_scale),
                (up_scale_hbm, up_scale),
                (conv_weight_hbm, conv_weight),
                (conv_bias_hbm, conv_bias),
                (down_scale_hbm, down_scale),
            )
        )
    ]
    pieces = [(g * size, size) for g in range(GROUPS)] + ([(main, rem)] if rem else [])
    early = [0] + list(range(GROUPS, len(pieces))) + list(range(1, GROUPS))

    def load(layer, kind, part):
        src, dst = ((gate_weight, stage_gate), (up_weight, stage_up))[kind]
        r = pl.ds(*pieces[part])
        return pltpu.make_async_copy(
            src.at[layer, r], dst.at[layer, r], load_sem.at[layer, kind * len(pieces) + part]
        )

    def load_out(layer):
        return pltpu.make_async_copy(
            down_weight.at[layer], stage_down.at[layer], load_sem.at[layer, 2 * len(pieces)]
        )

    for s in range(sequences):
        token_copy(s).start()
    smalls[0].start()
    for part in early:
        for kind in range(2):
            load(0, kind, part).start()
    for copy in smalls[1:]:
        copy.start()

    block = 32

    def convert_piece(layer, kind, part):
        load(layer, kind, part).wait()
        src = (stage_gate, stage_up)[kind]
        if part < GROUPS:
            shift = lines_in[part][0] + kind * size - part * size

            @pl.loop(part * size // block, (part + 1) * size // block)
            def _(i):
                r = pl.ds(pl.multiple_of(i * block, block), block)
                r2 = pl.ds(pl.multiple_of(shift + i * block, block), block)
                in_w[layer, r2, :] = src[layer, r, :].astype(jnp.bfloat16)

        else:
            first = 2 * size + kind * rem
            in_w[layer, first : first + rem, :] = src[layer, main:, :].astype(jnp.bfloat16)

    def convert_group(layer, g):
        for part in [g] + (list(range(GROUPS, len(pieces))) if g == 0 else []):
            for kind in range(2):
                convert_piece(layer, kind, part)
        if g == 0:
            first = 2 * size + 2 * rem
            in_w[layer, first : 2 * size + LANES, :] = jnp.zeros(
                (LANES - 2 * rem, width), jnp.bfloat16
            )

    def convert_in(layer):
        for g in range(GROUPS):
            convert_group(layer, g)

    def convert_out(layer):
        load_out(layer).wait()

        def rows_to(first, shift, count):
            @pl.loop(first // block, (first + count) // block)
            def _(i):
                r = pl.ds(pl.multiple_of(i * block, block), block)
                r2 = pl.ds(pl.multiple_of(shift + i * block, block), block)
                out_w[layer, r2, :half] = stage_down[layer, r, other_cols].astype(jnp.bfloat16)
                out_w[layer, r2, half:] = stage_down[layer, r, my_cols].astype(jnp.bfloat16)

        for g in range(GROUPS):
            rows_to(g * size, lines_hid[g][0] - g * size, size)
        if rem:
            rows_to(main, size - main, rem)
            out_w[layer, size + rem : size + LANES, :] = jnp.zeros(
                (LANES - rem, width), jnp.bfloat16
            )

    lane = lax.broadcasted_iota(jnp.int32, (1, LANES), 1)

    def put_squares(tile, squares):
        high = squares.astype(jnp.bfloat16).astype(jnp.float32)
        low = squares - high
        return jnp.where(lane == 2 * rem, high, jnp.where(lane == 2 * rem + 1, low, tile))

    def get_squares(tile):
        keep = jnp.logical_and(lane >= 2 * rem, lane < 2 * rem + 2)
        return jnp.sum(jnp.where(keep, tile, 0.0), axis=1, keepdims=True)

    def slot_of(k, kind):
        return k % WINDOW[kind] if isinstance(k, int) else lax.rem(k, WINDOW[kind])

    def launch(k, kind, copies, opens=True):
        if opens and not isinstance(k, int):

            @pl.when(k >= WINDOW[kind])
            def _():
                sent(k, kind)

        for copy in copies:
            copy.start()

    def take(ref, sem):
        pltpu.make_async_copy(ref, ref, sem).wait()

    def sent(k, kind):
        if kind == "near":
            take(own_part.at[k], near_s.at[slot_of(k, kind)])
        if kind == "far":
            take(far_send.at[k], far_s.at[slot_of(k, kind)])
        if kind == "hid":
            wide = (ra - 1) * main // sequences
            take(own_part.at[k, :, pl.ds(0, wide)], hid_s.at[slot_of(k, kind)])
            if rem:
                take(hid_rem.at[pl.ds(0, ra - 1), 0], rem_s.at[slot_of(k, kind)])
        if kind == "pair":
            take(pair_send.at[k], pair_s.at[slot_of(k, kind)])
        if kind == "chip":
            take(chip_part.at[k, pl.ds(0, chips - 1)], chip_s.at[slot_of(k, kind)])
        if kind == "out":
            take(state.at[k, :, my_cols], out_s.at[slot_of(k, kind)])

    def near_copy(k, first, g):
        to = jnp.where(me == 0, 1, 2)
        passed = jnp.where(me < 2, 1, 0)
        r = hid_rows(passed if first else 1 - passed)
        return pltpu.make_async_remote_copy(
            src_ref=own_part.at[k, r, pl.ds(*lines_in[g])],
            dst_ref=near_part.at[k, r, pl.ds(*lines_in[g])],
            send_sem=near_s.at[slot_of(k, "near")],
            recv_sem=near_r.at[slot_of(k, "near"), 2 * g + int(first)],
            device_id={"ra": to},
            device_id_type=MESH,
        )

    def far_copy(k, g):
        return pltpu.make_async_remote_copy(
            src_ref=far_send.at[k, :, pl.ds(*lines_in[g])],
            dst_ref=far_part.at[k, :, pl.ds(*lines_in[g])],
            send_sem=far_s.at[slot_of(k, "far")],
            recv_sem=far_r.at[slot_of(k, "far"), g],
            device_id={"ra": 3 - me},
            device_id_type=MESH,
        )

    def hid_rows(seq):
        return pl.ds(pl.multiple_of(seq * step, step), step)

    def hid_copy(k, d, seq, g):
        return pltpu.make_async_remote_copy(
            src_ref=hidden.at[k, hid_rows(seq), pl.ds(*lines_hid[g])],
            dst_ref=hidden.at[k, hid_rows(seq), pl.ds(*lines_hid[g])],
            send_sem=hid_s.at[slot_of(k, "hid")],
            recv_sem=hid_r.at[slot_of(k, "hid"), seq],
            device_id={"ra": lax.rem(me + d, ra)},
            device_id_type=MESH,
        )

    def rem_copy(k, d, seq):
        return pltpu.make_async_remote_copy(
            src_ref=hid_rem.at[k, seq],
            dst_ref=hid_rem.at[k, seq],
            send_sem=rem_s.at[slot_of(k, "hid")],
            recv_sem=rem_r.at[slot_of(k, "hid"), seq],
            device_id={"ra": lax.rem(me + d, ra)},
            device_id_type=MESH,
        )

    def pair_copy(k):
        return pltpu.make_async_remote_copy(
            src_ref=pair_send.at[k],
            dst_ref=pair_recv.at[k],
            send_sem=pair_s.at[slot_of(k, "pair")],
            recv_sem=pair_r.at[slot_of(k, "pair")],
            device_id={"cb": 2 * chip + 1 - core},
            device_id_type=MESH,
        )

    def chip_copy(k, d):
        return pltpu.make_async_remote_copy(
            src_ref=chip_part.at[k, chip],
            dst_ref=chip_part.at[k, chip],
            send_sem=chip_s.at[slot_of(k, "chip")],
            recv_sem=chip_r.at[slot_of(k, "chip")],
            device_id={"cb": 2 * lax.rem(chip + d, chips) + core},
            device_id_type=MESH,
        )

    def out_copy(k, cols):
        return pltpu.make_async_remote_copy(
            src_ref=state.at[k + chunks, :, cols],
            dst_ref=state.at[k + chunks, :, cols],
            send_sem=out_s.at[slot_of(k, "out")],
            recv_sem=out_r.at[slot_of(k, "out")],
            device_id={"cb": 2 * chip + 1 - core},
            device_id_type=MESH,
        )

    def scaled_rows(k):
        layer = k // chunks

        values = state[k].astype(jnp.float32)
        squares = jnp.sum(values * values, axis=1, keepdims=True)
        gain = norm_gain[pl.ds(layer, 1), :]
        return (values * gain).astype(jnp.bfloat16), squares

    def project(k, scaled, squares, g):
        layer = k // chunks
        begin, count = lines_in[g]
        cols = 512

        def product(start, stop):
            return lax.dot_general(
                scaled,
                in_w[layer, start:stop, :],
                (((1,), (1,)), ((), ())),
                preferred_element_type=jnp.float32,
            )

        plain = begin + 2 * size
        for start in range(begin, plain, cols):
            stop = min(start + cols, plain)
            own_part[k, :, start:stop] = product(start, stop).astype(jnp.bfloat16)
        if g == 0:
            tile = put_squares(product(plain, plain + LANES), squares)
            own_part[k, :, plain : plain + LANES] = tile.astype(jnp.bfloat16)

    def send_near(k, g, which=(True, False)):
        @pl.when(outer)
        def _():
            copies = [near_copy(k, first, g) for first in which]
            launch(k, "near", copies, g == 0 and which[0])

    def enter(k):
        @pl.when(k > 0)
        def _():
            scaled, squares = scaled_rows(k)
            for g in range(GROUPS):
                project(k, scaled, squares, g)
                send_near(k, g, (True,))
            for g in range(GROUPS):
                send_near(k, g, (False,))

    def mix(k):
        r = hid_rows(1 - own_seq)
        for g in range(GROUPS):
            near_copy(k, True, g).wait_recv()
            begin = lines_in[g][0]
            plain = begin + 2 * size

            def both(start, stop):
                return own_part[k, r, start:stop].astype(jnp.float32) + near_part[
                    k, r, start:stop
                ].astype(jnp.float32)

            far_send[k, :, begin:plain] = both(begin, plain).astype(jnp.bfloat16)
            if g == 0:
                tile = both(plain, plain + LANES)
                far_send[k, :, plain : plain + LANES] = put_squares(
                    tile, get_squares(tile)
                ).astype(jnp.bfloat16)
            launch(k, "far", [far_copy(k, g)], g == 0)

    def act(k):
        layer = k // chunks
        r = hid_rows(own_seq)

        def total(start, stop):
            return (
                own_part[k, r, start:stop].astype(jnp.float32)
                + near_part[k, r, start:stop].astype(jnp.float32)
                + far_part[k, :, start:stop].astype(jnp.float32)
            )

        @pl.when(k % chunks == 0)
        def _():
            conv_pad[0:8, :] = jnp.zeros((8, conv_pad.shape[1]), jnp.float32)

        def piece(inverse_rms, gate, up, start, stop):
            def param(row):
                return params[layer, row : row + 1, start:stop]

            conv_pad[8 : 8 + step, start:stop] = gate * inverse_rms * param(0)
            conv = param(2)
            taps = conv_weight.shape[0]
            for j in range(taps):
                first = 8 - (taps - 1) + j
                conv = conv + param(3 + j) * conv_pad[first : first + step, start:stop]
            conv_pad[0:8, start:stop] = conv_pad[step : step + 8, start:stop]
            value = conv / (1.0 + jnp.exp(-conv)) * (up * inverse_rms * param(1))
            return value

        cols = 256
        inverse_rms = None
        for g in range(GROUPS):
            near_copy(k, False, g).wait_recv()
            far_copy(k, g).wait_recv()
            begin, to = lines_in[g][0], lines_hid[g][0]
            if g == 0:
                tile = total(2 * size, 2 * size + LANES)
                inverse_rms = lax.rsqrt(get_squares(tile) / (width * ra) + eps)
                if rem:
                    up = pltpu.roll(tile, LANES - rem, axis=1)
                    value = piece(inverse_rms, tile, up, size, size + LANES)
                    packed = value[: step // 2] + pltpu.roll(value[step // 2 :], rem, axis=1)
                    hid_rem[k, own_seq] = packed.astype(jnp.bfloat16)
            for start in range(0, size, cols):
                stop = min(start + cols, size)
                gate = total(begin + start, begin + stop)
                up = total(begin + size + start, begin + size + stop)
                value = piece(inverse_rms, gate, up, to + start, to + stop)
                hidden[k, r, to + start : to + stop] = value.astype(jnp.bfloat16)
            copies = []
            for d in (2, 1, 3):
                if rem and g == 0:
                    copies.append(rem_copy(k, d, own_seq))
                copies.append(hid_copy(k, d, own_seq, g))
            launch(k, "hid", copies, g == 0)

    def down(k):
        layer = k // chunks
        for seq in range(sequences):

            @pl.when(jnp.logical_not(jnp.logical_and(inner, own_seq == seq)))
            def _():
                if rem:
                    rem_copy(k, 1, seq).wait_recv()
                r = hid_rows(seq)
                take(own_part.at[k, r, pl.ds(0, main)], hid_r.at[slot_of(k, "hid"), seq])

        if rem:
            for seq in range(sequences):
                packed = hid_rem[k, seq].astype(jnp.float32)
                for part in range(2):
                    first = seq * step + part * (step // 2)
                    rows_of[first : first + step // 2, :] = (
                        pltpu.roll(packed, LANES - rem, axis=1) if part else packed
                    )
            hidden[k, :, size : size + LANES] = rows_of[...].astype(jnp.bfloat16)
        value = jnp.dot(hidden[k], out_w[layer], preferred_element_type=jnp.float32)
        pair_send[k] = value[:, :half].astype(jnp.bfloat16)
        down_keep[k] = value[:, half:]
        launch(k, "pair", [pair_copy(k)])

    def pair(k):
        pair_copy(k).wait_recv()
        chip_part[k, chip] = (down_keep[k] + pair_recv[k].astype(jnp.float32)).astype(jnp.bfloat16)
        launch(k, "chip", [chip_copy(k, d) for d in range(1, chips)])

    def fold(k):
        layer = k // chunks
        take(chip_part.at[k, pl.ds(0, chips - 1)], chip_r.at[slot_of(k, "chip")])
        total = chip_part[k, 0].astype(jnp.float32)
        for g in range(1, chips):
            total = total + chip_part[k, g].astype(jnp.float32)
        kept = residual_keep * state[k, :, my_cols].astype(jnp.float32)
        scale = down_scale[pl.ds(layer, 1), my_cols]
        state[k + chunks, :, my_cols] = (kept + total * scale).astype(jnp.bfloat16)
        launch(k, "out", [out_copy(k, my_cols)])

    def done(k):
        out_copy(k, other_cols).wait_recv()

        @pl.when(k >= chunks)
        def _():
            for s in range(sequences):
                c = pl.ds(pl.multiple_of((k - chunks) * step, step), step)
                out[s, c, :] = state[k + chunks, s * step : (s + 1) * step, :]

    smalls[0].wait()
    for s in range(sequences):
        token_copy(s).wait()
    first_scaled, first_squares = scaled_rows(0)
    for g in range(GROUPS):
        convert_group(0, g)
        if g == GROUPS - 1:
            load_out(0).start()
            for part in early:
                for kind in range(2):
                    load(1, kind, part).start()
            load_out(1).start()
        project(0, first_scaled, first_squares, g)
        if g == 0:
            pl.semaphore_wait(barrier, jnp.where(inner, ra - 1, ra - 2) + chips)
        send_near(0, g)

    works = dict(
        enter=enter, mix=mix, act=act, down=down, pair=pair, fold=fold, done=done
    )

    def prepare():
        for copy in smalls[1:]:
            copy.wait()
        for layer in range(layers):
            lines = [gate_scale[layer : layer + 1, :], up_scale[layer : layer + 1, :]]
            lines.append(conv_bias[layer : layer + 1, :])
            lines += [conv_weight[j, layer : layer + 1, :] for j in range(conv_weight.shape[0])]
            for row, line in enumerate(lines):
                if rem:
                    zeros = jnp.zeros((1, LANES - rem), jnp.float32)
                    params[layer, row : row + 1, size : size + LANES] = jnp.concatenate(
                        [line[:, main:], zeros], axis=1
                    )
                for g in range(GROUPS):
                    to = lines_hid[g][0]
                    params[layer, row : row + 1, to : to + size] = line[
                        :, g * size : (g + 1) * size
                    ]

    @pl.loop(0, items + max(lag for _, lag in PLAN))
    def _(slot):
        for name, lag in PLAN:
            item = slot - lag
            good = jnp.logical_and(item >= 0, item < items)
            if name in ("mix", "act"):
                good = jnp.logical_and(good, inner)

            @pl.when(good)
            def _():
                works[name](item)

            if name == "enter":

                @pl.when(slot == 0)
                def _():
                    prepare()

                for at, (kind, layer) in CONVERT.items():

                    @pl.when(slot == at)
                    def _():
                        (convert_in if kind == "in" else convert_out)(layer)

    def drain(kind):
        @pl.loop(max(items - WINDOW[kind], 0), items)
        def _(k):
            sent(k, kind)

    @pl.when(outer)
    def _():
        drain("near")

    @pl.when(inner)
    def _():
        drain("far")
        drain("hid")

    for kind in ("pair", "chip", "out"):
        drain(kind)


def fused_shards(ra, cb, chunks, *operands):
    tokens, gate_weight = operands[0], operands[2]
    layers = 2
    sequences, length, width = tokens.shape
    units = gate_weight.shape[2]
    main = units // LANES * LANES
    total_cols = 2 * main + LANES
    padded = main + (LANES if units > main else 0)
    step = length // chunks
    rows = sequences * step
    items = layers * chunks
    half = width // 2
    chips = cb // 2
    taps = operands[6].shape[1]
    hbm = pl.BlockSpec(memory_space=pl.ANY)
    dma = pltpu.SemaphoreType.DMA
    bf16, f32 = jnp.bfloat16, jnp.float32
    return pl.pallas_call(
        functools.partial(fused, chunks, ra, cb),
        out_shape=pltpu.VMEM(tokens.shape, tokens.dtype),
        in_specs=[hbm] * 10,
        out_specs=pl.BlockSpec(memory_space=pltpu.VMEM),
        scratch_shapes=[
            pltpu.VMEM((layers, units, width), f32),
            pltpu.VMEM((layers, units, width), f32),
            pltpu.VMEM((layers, units, width), f32),
            pltpu.VMEM((layers, width), f32),
            pltpu.VMEM((layers, units), f32),
            pltpu.VMEM((layers, units), f32),
            pltpu.VMEM((taps, layers, units), f32),
            pltpu.VMEM((layers, units), f32),
            pltpu.VMEM((layers, width), f32),
            pltpu.VMEM((layers, total_cols, width), bf16),
            pltpu.VMEM((layers, padded, width), bf16),
            pltpu.VMEM((items + chunks, rows, width), bf16),
            pltpu.VMEM((items, rows, total_cols), bf16),
            pltpu.VMEM((items, rows, total_cols), bf16),
            pltpu.VMEM((items, step, total_cols), bf16),
            pltpu.VMEM((items, step, total_cols), bf16),
            pltpu.VMEM((items, rows, padded), bf16),
            pltpu.VMEM((items, sequences, step // 2, LANES), bf16),
            pltpu.VMEM((items, rows, half), f32),
            pltpu.VMEM((items, rows, half), bf16),
            pltpu.VMEM((items, rows, half), bf16),
            pltpu.VMEM((items, chips, rows, half), bf16),
            pltpu.VMEM((rows, LANES), f32),
            pltpu.VMEM((8 + step, padded), f32),
            pltpu.VMEM((layers, 3 + taps, padded), f32),
            dma((layers, 2 * GROUPS + 3)),
            dma((6,)),
            dma((sequences,)),
            dma((WINDOW["near"],)),
            dma((WINDOW["near"], 2 * GROUPS)),
            dma((WINDOW["far"],)),
            dma((WINDOW["far"], GROUPS)),
            dma((WINDOW["hid"],)),
            dma((WINDOW["hid"], sequences)),
            dma((WINDOW["hid"],)),
            dma((WINDOW["hid"], sequences)),
            dma((WINDOW["pair"],)),
            dma((WINDOW["pair"],)),
            dma((WINDOW["chip"],)),
            dma((WINDOW["chip"],)),
            dma((WINDOW["out"],)),
            dma((WINDOW["out"],)),
        ],
        compiler_params=pltpu.CompilerParams(
            collective_id=0, has_side_effects=True, vmem_limit_bytes=60 * 1024 * 1024
        ),
    )(
        tokens.reshape(sequences, chunks, step, width),
        operands[1],
        jnp.swapaxes(gate_weight, 1, 2),
        operands[3],
        jnp.swapaxes(operands[4], 1, 2),
        operands[5],
        jnp.swapaxes(operands[6], 0, 1),
        *operands[7:],
    )


def fits(ra, cb, chunks, shape, local_width, local_units):
    rem = local_units % LANES
    return (
        ra == 4
        and cb % 2 == 0
        and cb >= 4
        and shape[0] == 2
        and shape[1] % (chunks * 16) == 0
        and local_width % (2 * LANES) == 0
        and local_units % 32 == 0
        and 2 * rem + 2 <= LANES
        and local_units >= LANES * GROUPS
        and local_units // LANES % GROUPS == 0
    )


def either(ra, cb, *operands):
    tokens, gate_weight = operands[0], operands[2]
    if fits(ra, cb, CHUNKS, tokens.shape, tokens.shape[2], gate_weight.shape[2]):
        return fused_shards(ra, cb, CHUNKS, *operands)
    return shards(*operands)


def solution(mesh):
    in_specs = (
        P(None, None, "ra"),
        P(None, "ra"),
        P(None, "ra", "cb"),
        P(None, "cb"),
        P(None, "ra", "cb"),
        P(None, "cb"),
        P(None, None, "cb"),
        P(None, "cb"),
        P(None, "cb", "ra"),
        P(None, "ra"),
    )
    out_specs = P(None, None, "ra")
    return jax.shard_map(
        functools.partial(either, mesh.shape["ra"], mesh.shape["cb"]),
        mesh=mesh,
        in_specs=in_specs,
        out_specs=out_specs,
        check_vma=False,
    )
```

```python
import functools

import jax
import jax.numpy as jnp
from jax import lax
from jax.experimental import pallas as pl
from jax.experimental.pallas import tpu as pltpu
from jax.sharding import PartitionSpec as P

eps = 1e-06
residual_keep = 0.5


def causal_mix(gate_seq, conv_taps, conv_shift):
    count = conv_taps.shape[0]
    length = gate_seq.shape[1]
    padded = jnp.pad(gate_seq, ((0, 0), (count - 1, 0), (0, 0)))
    running = jnp.zeros_like(gate_seq) + conv_shift[None, None, :]
    for offset in range(count):
        running = (
            running + conv_taps[offset][None, None, :] * padded[:, offset : offset + length, :]
        )
    return running


def sublayer(current, norm_g, gate_w, gate_s, up_w, up_s, conv_taps, conv_shift, down_w, down_s):
    sequences, length, local_width = current.shape
    row_count = sequences * length
    values = current.astype(jnp.float32).reshape(row_count, local_width)
    squares = jnp.sum(values * values, axis=1)
    scaled = (values * norm_g[None, :]).astype(jnp.bfloat16)
    gate_part = jnp.dot(scaled, gate_w.astype(jnp.bfloat16), preferred_element_type=jnp.float32)
    up_part = jnp.dot(scaled, up_w.astype(jnp.bfloat16), preferred_element_type=jnp.float32)
    gate_sum, up_sum = (
        lax.psum_scatter(gate_part, "ra", scatter_dimension=1, tiled=True),
        lax.psum_scatter(up_part, "ra", scatter_dimension=1, tiled=True),
    )
    square_sum = lax.psum(squares, "ra")
    share_cols = gate_sum.shape[1]
    col_start = lax.axis_index("ra") * share_cols
    col_gate = lax.dynamic_slice_in_dim(gate_s, col_start, share_cols, 0)
    col_up = lax.dynamic_slice_in_dim(up_s, col_start, share_cols, 0)
    used_taps = lax.dynamic_slice_in_dim(conv_taps, col_start, share_cols, 1)
    used_shift = lax.dynamic_slice_in_dim(conv_shift, col_start, share_cols, 0)
    inverse_rms = lax.rsqrt(square_sum / (local_width * lax.axis_size("ra")) + eps)[:, None]
    gate_sum = gate_sum * inverse_rms * col_gate[None, :]
    up_sum = up_sum * inverse_rms * col_up[None, :]
    units = gate_sum.shape[1]
    conv_out = causal_mix(gate_sum.reshape(sequences, length, units), used_taps, used_shift)
    hidden_act = (jax.nn.silu(conv_out) * up_sum.reshape(sequences, length, units)).astype(
        jnp.bfloat16
    )
    hidden_act = hidden_act.reshape(row_count, units)
    hidden_act = lax.all_gather(hidden_act, "ra", axis=1, tiled=True)
    down_part = jnp.dot(hidden_act, down_w.astype(jnp.bfloat16), preferred_element_type=jnp.float32)
    down_sum = lax.psum(down_part, "cb")
    branch = down_sum * down_s[None, :]
    return (
        (residual_keep * values + branch)
        .astype(jnp.bfloat16)
        .reshape(sequences, length, local_width)
    )


def shards(
    tokens,
    norm_gain,
    gate_weight,
    gate_scale,
    up_weight,
    up_scale,
    conv_weight,
    conv_bias,
    down_weight,
    down_scale,
):
    current = tokens
    for layer_index in range(2):
        current = sublayer(
            current,
            norm_gain[layer_index],
            gate_weight[layer_index],
            gate_scale[layer_index],
            up_weight[layer_index],
            up_scale[layer_index],
            conv_weight[layer_index],
            conv_bias[layer_index],
            down_weight[layer_index],
            down_scale[layer_index],
        )
    return current


MESH = pl.DeviceIdType.MESH
LANES = 128
CHUNKS = 8
GROUPS = 2
PLAN = (
    ("done", 8),
    ("act", 3),
    ("fold", 7),
    ("enter", 0),
    ("mix", 1),
    ("pair", 5),
    ("down", 4),
)
WINDOW = dict(near=5, far=4, hid=5, pair=4, chip=6, out=2)
CONVERT = {2: ("out", 0), 4: ("in", 1), 7: ("out", 1)}


def fused(
    chunks,
    ra,
    cb,
    tokens_hbm,
    norm_gain_hbm,
    gate_weight,
    gate_scale_hbm,
    up_weight,
    up_scale_hbm,
    conv_weight_hbm,
    conv_bias_hbm,
    down_weight,
    down_scale_hbm,
    out,
    stage_gate,
    stage_up,
    stage_down,
    norm_gain,
    gate_scale,
    up_scale,
    conv_weight,
    conv_bias,
    down_scale,
    in_w,
    out_w,
    state,
    own_part,
    near_part,
    far_send,
    far_part,
    hidden,
    hid_rem,
    down_keep,
    pair_send,
    pair_recv,
    chip_part,
    rows_of,
    conv_pad,
    params,
    load_sem,
    small_sem,
    token_sem,
    near_s,
    near_r,
    far_s,
    far_r,
    hid_s,
    hid_r,
    rem_s,
    rem_r,
    pair_s,
    pair_r,
    chip_s,
    chip_r,
    out_s,
    out_r,
):
    layers = 2
    sequences, _, step, width = tokens_hbm.shape
    units = gate_weight.shape[1]
    main = units // LANES * LANES
    rem = units - main
    total_cols = 2 * main + LANES
    rows = sequences * step
    items = layers * chunks
    half = width // 2
    chips = cb // 2
    size = main // GROUPS
    lines_in = [(0, 2 * size + LANES)]
    lines_hid = [(0, size)]
    for g in range(1, GROUPS):
        lines_in.append((sum(lines_in[-1]), 2 * size))
        lines_hid.append((g * size + (LANES if rem else 0), size))
    me = lax.axis_index("ra")
    mine = lax.axis_index("cb")
    core = lax.rem(mine, 2)
    chip = mine // 2
    others = [lax.rem(chip + d, chips) for d in range(1, chips)]
    if chips == 4:
        others = [3 - chip, chip + 1 - 2 * lax.rem(chip, 2), lax.rem(chip + 2, 4)]
    inner = jnp.logical_and(me >= 1, me <= 2)
    outer = jnp.logical_not(inner)
    own_seq = me - 1
    my_cols = pl.ds(pl.multiple_of(core * half, LANES), half)
    other_cols = pl.ds(pl.multiple_of((1 - core) * half, LANES), half)

    barrier = pltpu.get_barrier_semaphore()
    for d in range(1, ra):
        to = lax.rem(me + d, ra)

        @pl.when(jnp.logical_or(inner, jnp.logical_and(to >= 1, to <= 2)))
        def _():
            pl.semaphore_signal(barrier, inc=1, device_id={"ra": to}, device_id_type=MESH)

    pl.semaphore_signal(
        barrier, inc=1, device_id={"cb": 2 * chip + 1 - core}, device_id_type=MESH
    )
    for d in range(1, chips):
        pl.semaphore_signal(
            barrier,
            inc=1,
            device_id={"cb": 2 * lax.rem(chip + d, chips) + core},
            device_id_type=MESH,
        )

    def token_copy(s):
        return pltpu.make_async_copy(
            tokens_hbm.at[s],
            state.at[pl.ds(0, chunks), pl.ds(s * step, step)],
            token_sem.at[s],
        )

    smalls = [
        pltpu.make_async_copy(src, dst, small_sem.at[i])
        for i, (src, dst) in enumerate(
            (
                (norm_gain_hbm, norm_gain),
                (gate_scale_hbm, gate_scale),
                (up_scale_hbm, up_scale),
                (conv_weight_hbm, conv_weight),
                (conv_bias_hbm, conv_bias),
                (down_scale_hbm, down_scale),
            )
        )
    ]
    pieces = [(g * size, size) for g in range(GROUPS)] + ([(main, rem)] if rem else [])
    early = [0] + list(range(GROUPS, len(pieces))) + list(range(1, GROUPS))

    def load(layer, kind, part):
        src, dst = ((gate_weight, stage_gate), (up_weight, stage_up))[kind]
        r = pl.ds(*pieces[part])
        return pltpu.make_async_copy(
            src.at[layer, r], dst.at[layer, r], load_sem.at[layer, kind * len(pieces) + part]
        )

    def load_out(layer):
        return pltpu.make_async_copy(
            down_weight.at[layer], stage_down.at[layer], load_sem.at[layer, 2 * len(pieces)]
        )

    for s in range(sequences):
        token_copy(s).start()
    smalls[0].start()
    for part in early:
        for kind in range(2):
            load(0, kind, part).start()
    for copy in smalls[1:]:
        copy.start()

    block = 32

    def convert_piece(layer, kind, part):
        load(layer, kind, part).wait()
        src = (stage_gate, stage_up)[kind]
        if part < GROUPS:
            shift = lines_in[part][0] + kind * size - part * size

            @pl.loop(part * size // block, (part + 1) * size // block)
            def _(i):
                r = pl.ds(pl.multiple_of(i * block, block), block)
                r2 = pl.ds(pl.multiple_of(shift + i * block, block), block)
                in_w[layer, r2, :] = src[layer, r, :].astype(jnp.bfloat16)

        else:
            first = 2 * size + kind * rem
            in_w[layer, first : first + rem, :] = src[layer, main:, :].astype(jnp.bfloat16)

    def convert_group(layer, g):
        for part in [g] + (list(range(GROUPS, len(pieces))) if g == 0 else []):
            for kind in range(2):
                convert_piece(layer, kind, part)
        if g == 0:
            first = 2 * size + 2 * rem
            in_w[layer, first : 2 * size + LANES, :] = jnp.zeros(
                (LANES - 2 * rem, width), jnp.bfloat16
            )

    def convert_in(layer):
        for g in range(GROUPS):
            convert_group(layer, g)

    def convert_out(layer):
        load_out(layer).wait()

        def rows_to(first, shift, count):
            @pl.loop(first // block, (first + count) // block)
            def _(i):
                r = pl.ds(pl.multiple_of(i * block, block), block)
                r2 = pl.ds(pl.multiple_of(shift + i * block, block), block)
                out_w[layer, r2, :half] = stage_down[layer, r, other_cols].astype(jnp.bfloat16)
                out_w[layer, r2, half:] = stage_down[layer, r, my_cols].astype(jnp.bfloat16)

        for g in range(GROUPS):
            rows_to(g * size, lines_hid[g][0] - g * size, size)
        if rem:
            rows_to(main, size - main, rem)
            out_w[layer, size + rem : size + LANES, :] = jnp.zeros(
                (LANES - rem, width), jnp.bfloat16
            )

    lane = lax.broadcasted_iota(jnp.int32, (1, LANES), 1)

    def put_squares(tile, squares):
        high = squares.astype(jnp.bfloat16).astype(jnp.float32)
        low = squares - high
        return jnp.where(lane == 2 * rem, high, jnp.where(lane == 2 * rem + 1, low, tile))

    def get_squares(tile):
        keep = jnp.logical_and(lane >= 2 * rem, lane < 2 * rem + 2)
        return jnp.sum(jnp.where(keep, tile, 0.0), axis=1, keepdims=True)

    def slot_of(k, kind):
        return k % WINDOW[kind] if isinstance(k, int) else lax.rem(k, WINDOW[kind])

    def launch(k, kind, copies, opens=True):
        if opens and not isinstance(k, int):

            @pl.when(k >= WINDOW[kind])
            def _():
                sent(k, kind)

        for copy in copies:
            copy.start()

    def take(ref, sem):
        pltpu.make_async_copy(ref, ref, sem).wait()

    def sent(k, kind):
        if kind == "near":
            take(own_part.at[k], near_s.at[slot_of(k, kind)])
        if kind == "far":
            take(far_send.at[k], far_s.at[slot_of(k, kind)])
        if kind == "hid":
            wide = (ra - 1) * main // sequences
            take(own_part.at[k, :, pl.ds(0, wide)], hid_s.at[slot_of(k, kind)])
            if rem:
                take(hid_rem.at[pl.ds(0, ra - 1), 0], rem_s.at[slot_of(k, kind)])
        if kind == "pair":
            take(pair_send.at[k], pair_s.at[slot_of(k, kind)])
        if kind == "chip":
            take(chip_part.at[k, pl.ds(0, chips - 1)], chip_s.at[slot_of(k, kind)])
        if kind == "out":
            take(state.at[k, :, my_cols], out_s.at[slot_of(k, kind)])

    def near_copy(k, first, g):
        to = jnp.where(me == 0, 1, 2)
        passed = jnp.where(me < 2, 1, 0)
        r = hid_rows(passed if first else 1 - passed)
        return pltpu.make_async_remote_copy(
            src_ref=own_part.at[k, r, pl.ds(*lines_in[g])],
            dst_ref=near_part.at[k, r, pl.ds(*lines_in[g])],
            send_sem=near_s.at[slot_of(k, "near")],
            recv_sem=near_r.at[slot_of(k, "near"), 2 * g + int(first)],
            device_id={"ra": to},
            device_id_type=MESH,
        )

    def far_copy(k, g):
        return pltpu.make_async_remote_copy(
            src_ref=far_send.at[k, :, pl.ds(*lines_in[g])],
            dst_ref=far_part.at[k, :, pl.ds(*lines_in[g])],
            send_sem=far_s.at[slot_of(k, "far")],
            recv_sem=far_r.at[slot_of(k, "far"), g],
            device_id={"ra": 3 - me},
            device_id_type=MESH,
        )

    def hid_rows(seq):
        return pl.ds(pl.multiple_of(seq * step, step), step)

    def hid_copy(k, d, seq, g):
        return pltpu.make_async_remote_copy(
            src_ref=hidden.at[k, hid_rows(seq), pl.ds(*lines_hid[g])],
            dst_ref=hidden.at[k, hid_rows(seq), pl.ds(*lines_hid[g])],
            send_sem=hid_s.at[slot_of(k, "hid")],
            recv_sem=hid_r.at[slot_of(k, "hid"), seq],
            device_id={"ra": lax.rem(me + d, ra)},
            device_id_type=MESH,
        )

    def rem_copy(k, d, seq):
        return pltpu.make_async_remote_copy(
            src_ref=hid_rem.at[k, seq],
            dst_ref=hid_rem.at[k, seq],
            send_sem=rem_s.at[slot_of(k, "hid")],
            recv_sem=rem_r.at[slot_of(k, "hid"), seq],
            device_id={"ra": lax.rem(me + d, ra)},
            device_id_type=MESH,
        )

    def pair_copy(k):
        return pltpu.make_async_remote_copy(
            src_ref=pair_send.at[k],
            dst_ref=pair_recv.at[k],
            send_sem=pair_s.at[slot_of(k, "pair")],
            recv_sem=pair_r.at[slot_of(k, "pair")],
            device_id={"cb": 2 * chip + 1 - core},
            device_id_type=MESH,
        )

    def chip_copy(k, d):
        return pltpu.make_async_remote_copy(
            src_ref=chip_part.at[k, chip],
            dst_ref=chip_part.at[k, chip],
            send_sem=chip_s.at[slot_of(k, "chip")],
            recv_sem=chip_r.at[slot_of(k, "chip")],
            device_id={"cb": 2 * others[d - 1] + core},
            device_id_type=MESH,
        )

    def out_copy(k, cols):
        return pltpu.make_async_remote_copy(
            src_ref=state.at[k + chunks, :, cols],
            dst_ref=state.at[k + chunks, :, cols],
            send_sem=out_s.at[slot_of(k, "out")],
            recv_sem=out_r.at[slot_of(k, "out")],
            device_id={"cb": 2 * chip + 1 - core},
            device_id_type=MESH,
        )

    def scaled_rows(k):
        layer = k // chunks

        values = state[k].astype(jnp.float32)
        squares = jnp.sum(values * values, axis=1, keepdims=True)
        gain = norm_gain[pl.ds(layer, 1), :]
        return (values * gain).astype(jnp.bfloat16), squares

    def project(k, scaled, squares, g):
        layer = k // chunks
        begin, count = lines_in[g]
        cols = 512

        def product(start, stop):
            return lax.dot_general(
                scaled,
                in_w[layer, start:stop, :],
                (((1,), (1,)), ((), ())),
                preferred_element_type=jnp.float32,
            )

        plain = begin + 2 * size
        for start in range(begin, plain, cols):
            stop = min(start + cols, plain)
            own_part[k, :, start:stop] = product(start, stop).astype(jnp.bfloat16)
        if g == 0:
            tile = put_squares(product(plain, plain + LANES), squares)
            own_part[k, :, plain : plain + LANES] = tile.astype(jnp.bfloat16)

    def send_near(k, g, which=(True, False)):
        @pl.when(outer)
        def _():
            copies = [near_copy(k, first, g) for first in which]
            launch(k, "near", copies, g == 0 and which[0])

    def enter(k):
        @pl.when(k > 0)
        def _():
            scaled, squares = scaled_rows(k)
            for g in range(GROUPS):
                project(k, scaled, squares, g)
                send_near(k, g, (True,))
            for g in range(GROUPS):
                send_near(k, g, (False,))

    def mix(k):
        r = hid_rows(1 - own_seq)
        for g in range(GROUPS):
            near_copy(k, True, g).wait_recv()
            begin = lines_in[g][0]
            plain = begin + 2 * size

            def both(start, stop):
                return own_part[k, r, start:stop].astype(jnp.float32) + near_part[
                    k, r, start:stop
                ].astype(jnp.float32)

            far_send[k, :, begin:plain] = both(begin, plain).astype(jnp.bfloat16)
            if g == 0:
                tile = both(plain, plain + LANES)
                far_send[k, :, plain : plain + LANES] = put_squares(
                    tile, get_squares(tile)
                ).astype(jnp.bfloat16)
            launch(k, "far", [far_copy(k, g)], g == 0)

    def act(k):
        layer = k // chunks
        r = hid_rows(own_seq)

        def total(start, stop):
            return (
                own_part[k, r, start:stop].astype(jnp.float32)
                + near_part[k, r, start:stop].astype(jnp.float32)
                + far_part[k, :, start:stop].astype(jnp.float32)
            )

        @pl.when(k % chunks == 0)
        def _():
            conv_pad[0:8, :] = jnp.zeros((8, conv_pad.shape[1]), jnp.float32)

        def piece(inverse_rms, gate, up, start, stop):
            def param(row):
                return params[layer, row : row + 1, start:stop]

            conv_pad[8 : 8 + step, start:stop] = gate * inverse_rms * param(0)
            conv = param(2)
            taps = conv_weight.shape[0]
            for j in range(taps):
                first = 8 - (taps - 1) + j
                conv = conv + param(3 + j) * conv_pad[first : first + step, start:stop]
            conv_pad[0:8, start:stop] = conv_pad[step : step + 8, start:stop]
            value = conv / (1.0 + jnp.exp(-conv)) * (up * inverse_rms * param(1))
            return value

        cols = 256
        inverse_rms = None
        for g in range(GROUPS):
            near_copy(k, False, g).wait_recv()
            far_copy(k, g).wait_recv()
            begin, to = lines_in[g][0], lines_hid[g][0]
            if g == 0:
                tile = total(2 * size, 2 * size + LANES)
                inverse_rms = lax.rsqrt(get_squares(tile) / (width * ra) + eps)
                if rem:
                    up = pltpu.roll(tile, LANES - rem, axis=1)
                    value = piece(inverse_rms, tile, up, size, size + LANES)
                    packed = value[: step // 2] + pltpu.roll(value[step // 2 :], rem, axis=1)
                    hid_rem[k, own_seq] = packed.astype(jnp.bfloat16)
            for start in range(0, size, cols):
                stop = min(start + cols, size)
                gate = total(begin + start, begin + stop)
                up = total(begin + size + start, begin + size + stop)
                value = piece(inverse_rms, gate, up, to + start, to + stop)
                hidden[k, r, to + start : to + stop] = value.astype(jnp.bfloat16)
            copies = []
            for d in (2, 1, 3):
                if rem and g == 0:
                    copies.append(rem_copy(k, d, own_seq))
                copies.append(hid_copy(k, d, own_seq, g))
            launch(k, "hid", copies, g == 0)

    def down(k):
        layer = k // chunks
        for seq in range(sequences):

            @pl.when(jnp.logical_not(jnp.logical_and(inner, own_seq == seq)))
            def _():
                if rem:
                    rem_copy(k, 1, seq).wait_recv()
                r = hid_rows(seq)
                take(own_part.at[k, r, pl.ds(0, main)], hid_r.at[slot_of(k, "hid"), seq])

        if rem:
            for seq in range(sequences):
                packed = hid_rem[k, seq].astype(jnp.float32)
                for part in range(2):
                    first = seq * step + part * (step // 2)
                    rows_of[first : first + step // 2, :] = (
                        pltpu.roll(packed, LANES - rem, axis=1) if part else packed
                    )
            hidden[k, :, size : size + LANES] = rows_of[...].astype(jnp.bfloat16)
        value = jnp.dot(hidden[k], out_w[layer], preferred_element_type=jnp.float32)
        pair_send[k] = value[:, :half].astype(jnp.bfloat16)
        down_keep[k] = value[:, half:]
        launch(k, "pair", [pair_copy(k)])

    def pair(k):
        pair_copy(k).wait_recv()
        chip_part[k, chip] = (down_keep[k] + pair_recv[k].astype(jnp.float32)).astype(jnp.bfloat16)
        launch(k, "chip", [chip_copy(k, d) for d in range(1, chips)])

    def fold(k):
        layer = k // chunks
        take(chip_part.at[k, pl.ds(0, chips - 1)], chip_r.at[slot_of(k, "chip")])
        total = chip_part[k, 0].astype(jnp.float32)
        for g in range(1, chips):
            total = total + chip_part[k, g].astype(jnp.float32)
        kept = residual_keep * state[k, :, my_cols].astype(jnp.float32)
        scale = down_scale[pl.ds(layer, 1), my_cols]
        state[k + chunks, :, my_cols] = (kept + total * scale).astype(jnp.bfloat16)
        launch(k, "out", [out_copy(k, my_cols)])

    def done(k):
        out_copy(k, other_cols).wait_recv()

        @pl.when(k >= chunks)
        def _():
            for s in range(sequences):
                c = pl.ds(pl.multiple_of((k - chunks) * step, step), step)
                out[s, c, :] = state[k + chunks, s * step : (s + 1) * step, :]

    smalls[0].wait()
    for s in range(sequences):
        token_copy(s).wait()
    first_scaled, first_squares = scaled_rows(0)
    for g in range(GROUPS):
        convert_group(0, g)
        if g == GROUPS - 1:
            load_out(0).start()
            for part in early:
                for kind in range(2):
                    load(1, kind, part).start()
            load_out(1).start()
        project(0, first_scaled, first_squares, g)
        if g == 0:
            pl.semaphore_wait(barrier, jnp.where(inner, ra - 1, ra - 2) + chips)
        send_near(0, g)

    works = dict(
        enter=enter, mix=mix, act=act, down=down, pair=pair, fold=fold, done=done
    )

    def prepare():
        for copy in smalls[1:]:
            copy.wait()
        for layer in range(layers):
            lines = [gate_scale[layer : layer + 1, :], up_scale[layer : layer + 1, :]]
            lines.append(conv_bias[layer : layer + 1, :])
            lines += [conv_weight[j, layer : layer + 1, :] for j in range(conv_weight.shape[0])]
            for row, line in enumerate(lines):
                if rem:
                    zeros = jnp.zeros((1, LANES - rem), jnp.float32)
                    params[layer, row : row + 1, size : size + LANES] = jnp.concatenate(
                        [line[:, main:], zeros], axis=1
                    )
                for g in range(GROUPS):
                    to = lines_hid[g][0]
                    params[layer, row : row + 1, to : to + size] = line[
                        :, g * size : (g + 1) * size
                    ]

    @pl.loop(0, items + max(lag for _, lag in PLAN))
    def _(slot):
        for name, lag in PLAN:
            item = slot - lag
            good = jnp.logical_and(item >= 0, item < items)
            if name in ("mix", "act"):
                good = jnp.logical_and(good, inner)

            @pl.when(good)
            def _():
                works[name](item)

            if name == "enter":

                @pl.when(slot == 0)
                def _():
                    prepare()

                for at, (kind, layer) in CONVERT.items():

                    @pl.when(slot == at)
                    def _():
                        (convert_in if kind == "in" else convert_out)(layer)

    def drain(kind):
        @pl.loop(max(items - WINDOW[kind], 0), items)
        def _(k):
            sent(k, kind)

    @pl.when(outer)
    def _():
        drain("near")

    @pl.when(inner)
    def _():
        drain("far")
        drain("hid")

    for kind in ("pair", "chip", "out"):
        drain(kind)


def fused_shards(ra, cb, chunks, *operands):
    tokens, gate_weight = operands[0], operands[2]
    layers = 2
    sequences, length, width = tokens.shape
    units = gate_weight.shape[2]
    main = units // LANES * LANES
    total_cols = 2 * main + LANES
    padded = main + (LANES if units > main else 0)
    step = length // chunks
    rows = sequences * step
    items = layers * chunks
    half = width // 2
    chips = cb // 2
    taps = operands[6].shape[1]
    hbm = pl.BlockSpec(memory_space=pl.ANY)
    dma = pltpu.SemaphoreType.DMA
    bf16, f32 = jnp.bfloat16, jnp.float32
    return pl.pallas_call(
        functools.partial(fused, chunks, ra, cb),
        out_shape=pltpu.VMEM(tokens.shape, tokens.dtype),
        in_specs=[hbm] * 10,
        out_specs=pl.BlockSpec(memory_space=pltpu.VMEM),
        scratch_shapes=[
            pltpu.VMEM((layers, units, width), f32),
            pltpu.VMEM((layers, units, width), f32),
            pltpu.VMEM((layers, units, width), f32),
            pltpu.VMEM((layers, width), f32),
            pltpu.VMEM((layers, units), f32),
            pltpu.VMEM((layers, units), f32),
            pltpu.VMEM((taps, layers, units), f32),
            pltpu.VMEM((layers, units), f32),
            pltpu.VMEM((layers, width), f32),
            pltpu.VMEM((layers, total_cols, width), bf16),
            pltpu.VMEM((layers, padded, width), bf16),
            pltpu.VMEM((items + chunks, rows, width), bf16),
            pltpu.VMEM((items, rows, total_cols), bf16),
            pltpu.VMEM((items, rows, total_cols), bf16),
            pltpu.VMEM((items, step, total_cols), bf16),
            pltpu.VMEM((items, step, total_cols), bf16),
            pltpu.VMEM((items, rows, padded), bf16),
            pltpu.VMEM((items, sequences, step // 2, LANES), bf16),
            pltpu.VMEM((items, rows, half), f32),
            pltpu.VMEM((items, rows, half), bf16),
            pltpu.VMEM((items, rows, half), bf16),
            pltpu.VMEM((items, chips, rows, half), bf16),
            pltpu.VMEM((rows, LANES), f32),
            pltpu.VMEM((8 + step, padded), f32),
            pltpu.VMEM((layers, 3 + taps, padded), f32),
            dma((layers, 2 * GROUPS + 3)),
            dma((6,)),
            dma((sequences,)),
            dma((WINDOW["near"],)),
            dma((WINDOW["near"], 2 * GROUPS)),
            dma((WINDOW["far"],)),
            dma((WINDOW["far"], GROUPS)),
            dma((WINDOW["hid"],)),
            dma((WINDOW["hid"], sequences)),
            dma((WINDOW["hid"],)),
            dma((WINDOW["hid"], sequences)),
            dma((WINDOW["pair"],)),
            dma((WINDOW["pair"],)),
            dma((WINDOW["chip"],)),
            dma((WINDOW["chip"],)),
            dma((WINDOW["out"],)),
            dma((WINDOW["out"],)),
        ],
        compiler_params=pltpu.CompilerParams(
            collective_id=0, has_side_effects=True, vmem_limit_bytes=60 * 1024 * 1024
        ),
    )(
        tokens.reshape(sequences, chunks, step, width),
        operands[1],
        jnp.swapaxes(gate_weight, 1, 2),
        operands[3],
        jnp.swapaxes(operands[4], 1, 2),
        operands[5],
        jnp.swapaxes(operands[6], 0, 1),
        *operands[7:],
    )


def fits(ra, cb, chunks, shape, local_width, local_units):
    rem = local_units % LANES
    return (
        ra == 4
        and cb % 2 == 0
        and cb >= 4
        and shape[0] == 2
        and shape[1] % (chunks * 16) == 0
        and local_width % (2 * LANES) == 0
        and local_units % 32 == 0
        and 2 * rem + 2 <= LANES
        and local_units >= LANES * GROUPS
        and local_units // LANES % GROUPS == 0
    )


def either(ra, cb, *operands):
    tokens, gate_weight = operands[0], operands[2]
    if fits(ra, cb, CHUNKS, tokens.shape, tokens.shape[2], gate_weight.shape[2]):
        return fused_shards(ra, cb, CHUNKS, *operands)
    return shards(*operands)


def solution(mesh):
    in_specs = (
        P(None, None, "ra"),
        P(None, "ra"),
        P(None, "ra", "cb"),
        P(None, "cb"),
        P(None, "ra", "cb"),
        P(None, "cb"),
        P(None, None, "cb"),
        P(None, "cb"),
        P(None, "cb", "ra"),
        P(None, "ra"),
    )
    out_specs = P(None, None, "ra")
    return jax.shard_map(
        functools.partial(either, mesh.shape["ra"], mesh.shape["cb"]),
        mesh=mesh,
        in_specs=in_specs,
        out_specs=out_specs,
        check_vma=False,
    )
```
